512 devices in a mesh: sp: 64 (over z, y), fs: 4 (over x), tp: 2 (over core).
Axes of the slice: x: 4, y: 8, z: 8, core: 2. Of those that a mesh axis runs over, the one named last changes fastest.
Arguments:
- tokens: bfloat16 [32768, 2048], P(('fs', 'sp')), parts along dimension 0, may hold values from -6 to 6
- norm_gain: bfloat16 [2048], replicated, may hold values from 0.099609375 to 1.8984375
- query_down: bfloat16 [2048, 512], P('sp'), may hold values from -0.125 to 0.125
- query_gain: bfloat16 [512], replicated, may hold values from 0.099609375 to 1.8984375
- latent_down: bfloat16 [2048, 256], replicated, may hold values from -0.125 to 0.125
- latent_gain: bfloat16 [256], replicated, may hold values from 0.099609375 to 1.8984375
- rope_down: bfloat16 [2048, 64], replicated, may hold values from -30 to 30
- query_up: bfloat16 [512, 1536], P(None, 'tp'), may hold values from -0.25 to 0.25
- key_up: bfloat16 [256, 1024], P(None, 'tp'), may hold values from -0.75 to 0.75
- value_up: bfloat16 [256, 1024], P(None, 'tp'), may hold values from -0.375 to 0.375
- glu_value: bfloat16 [2048, 1024], P('sp', 'tp'), may hold values from -0.125 to 0.125
- glu_gate: bfloat16 [2048, 1024], P('sp', 'tp'), may hold values from -0.125 to 0.125
- conv_taps: bfloat16 [31, 1024], P(None, 'tp'), may hold values from -1 to 1
- group_gain: bfloat16 [1024], P('tp'), may hold values from 0.099609375 to 1.8984375
- head_proj: bfloat16 [1024, 2048], P('tp', 'sp'), may hold values from -0.75 to 0.75
- channel_proj: bfloat16 [1024, 2048], P('tp', 'sp'), may hold values from -0.1875 to 0.1875
Outputs:
- mixed_out: bfloat16 [32768, 2048], P(('fs', 'sp'), 'tp'), parts along dimension 0
- log_weight: float32 [8, 32768], P('tp', ('fs', 'sp')), parts along dimension 1
The draws below stay inside these ranges and needn't reach their ends.
There are 4 independent parts, one for each index of `fs`. The reference program is written for one: setup_inputs(seed, part) draws one part's arguments, and reference() takes and returns one part's arrays. A program takes and returns all parts, laid end to end along the dimension named above; an argument that names none is the same for every part. Nothing has to cross between parts.
All inputs are finite; a program needn't handle non-finite values.
Results may differ from the reference program's by a relative error of at most 0.015.
The reference program's roundings to bfloat16 on the way count: a program that leaves them out, or rounds other values in their place, can miss the bound.
Values may be sent and summed in bfloat16 or wider, within the bound.
A program may use at most 128 MiB of HBM per device.

```python
import jax
import jax.numpy as jnp
from jax import lax

D = 2048
HEADS = 8
NOPE = 128
ROPE = 64
VDIM = 128
QR = 512
KVR = 256
CH = 1024
GROUPS = 8
WIDTH = 31
GRID_W = 64
TOK_DEV = 128
LENGTH = 8192
N_TP = 2


def draw_rope_down(key, part):
    base_key = jax.random.fold_in(jax.random.fold_in(key, 11), 0)
    entries = jax.random.normal(base_key, (D, ROPE), jnp.float32) * D ** (-0.5)
    return jnp.clip(entries, -30.0, 30.0).astype(jnp.bfloat16)


def steps_of(key, extent, cuts, least, high):
    factor_of, own = 1.0, jax.random.fold_in(key, 6)
    for position, blocks in cuts:
        steps = jnp.exp(jax.random.uniform(jax.random.fold_in(own, position), (blocks,), jnp.float32, least / len(cuts), high / len(cuts)))
        factor_of = factor_of * jnp.repeat(steps, extent[position] // blocks).reshape([-1 if axis == position else 1 for axis in range(len(extent))])
    return factor_of


def bell_draw(stream_key, extent, width, bound, cuts=(), held_as=jnp.bfloat16):
    loudness = steps_of(stream_key, extent, cuts, -0.22, 0.18) if cuts else 1.0
    drawn = jax.random.normal(stream_key, extent, jnp.float32) * width * loudness
    return jnp.minimum(jnp.maximum(drawn, -bound), bound).astype(held_as)


def setup_inputs(seed: int = 0, part: int = 0) -> dict:
    arg_keys = jax.random.split(jax.random.key(seed), 17)
    part_splits = jax.random.split(jax.random.fold_in(arg_keys[16], part), 17)
    tokens = bell_draw(part_splits[0], (LENGTH, D), 1.0, 6.0, ((0, 64),))
    norm_gain = jnp.clip(1.0 + 0.18 * jax.random.normal(arg_keys[1], (D,), jnp.float32), 0.099609375, 1.8984375).astype(jnp.bfloat16)
    query_down = bell_draw(arg_keys[2], (D, QR), D ** -0.5, 0.125, ((0, 64),))
    query_gain = jnp.clip(1.0 + 0.18 * jax.random.normal(arg_keys[3], (QR,), jnp.float32), 0.099609375, 1.8984375).astype(jnp.bfloat16)
    latent_down = bell_draw(arg_keys[4], (D, KVR), D ** -0.5, 0.125)
    latent_gain = jnp.clip(1.0 + 0.18 * jax.random.normal(arg_keys[5], (KVR,), jnp.float32), 0.099609375, 1.8984375).astype(jnp.bfloat16)
    rope_down = draw_rope_down(jax.random.fold_in(arg_keys[16], 71), part)
    query_up = bell_draw(arg_keys[7], (QR, HEADS * (NOPE + ROPE)), QR ** -0.5, 0.25, ((1, 2),))
    key_up = bell_draw(arg_keys[8], (KVR, HEADS * NOPE), 0.125, 0.75, ((1, 2),))
    value_up = bell_draw(arg_keys[9], (KVR, HEADS * VDIM), KVR ** -0.5, 0.375, ((1, 2),))
    glu_value = bell_draw(arg_keys[10], (D, CH), D ** -0.5, 0.125, ((0, 64), (1, 2)))
    glu_gate = bell_draw(arg_keys[11], (D, CH), D ** -0.5, 0.125, ((0, 64), (1, 2)))
    conv_taps = bell_draw(arg_keys[12], (WIDTH, CH), WIDTH ** -0.5, 1.0, ((1, 2),))
    group_gain = jnp.clip(1.0 + 0.18 * jax.random.normal(arg_keys[13], (CH,), jnp.float32), 0.099609375, 1.8984375).astype(jnp.bfloat16)
    head_proj = bell_draw(arg_keys[14], (HEADS * VDIM, D), (HEADS * VDIM // 16) ** -0.5, 0.75, ((0, 2), (1, 64)))
    channel_proj = bell_draw(arg_keys[15], (CH, D), CH ** -0.5, 0.1875, ((0, 2), (1, 64)))
    return {"tokens": tokens, "norm_gain": norm_gain, "query_down": query_down, "query_gain": query_gain, "latent_down": latent_down, "latent_gain": latent_gain, "rope_down": rope_down, "query_up": query_up, "key_up": key_up, "value_up": value_up, "glu_value": glu_value, "glu_gate": glu_gate, "conv_taps": conv_taps, "group_gain": group_gain, "head_proj": head_proj, "channel_proj": channel_proj}


norm_eps = 1e-06
rope_base = 10000.0

def rounded(values):
    return lax.optimization_barrier(values.astype(jnp.bfloat16))

def rms_scale(values, scale_gain):
    inv_rms = lax.rsqrt(lax.optimization_barrier(jnp.mean(values * values, axis=-1, keepdims=True)) + norm_eps)
    return values * inv_rms * scale_gain.astype(jnp.float32)

def angles_for(positions, rope_size):
    quarter = rope_size // 4
    inverse = rope_base ** (-jnp.arange(quarter, dtype=jnp.float32) / quarter)
    grid_row = (positions // GRID_W).astype(jnp.float32)
    grid_col = (positions % GRID_W).astype(jnp.float32)
    return jnp.concatenate([grid_row[:, None] * inverse, grid_col[:, None] * inverse], axis=-1)

def rotate(values, angles):
    half_size = values.shape[-1] // 2
    front_half = values[..., :half_size]
    back_half = values[..., half_size:]
    cosine = jnp.cos(angles)
    sine_part = jnp.sin(angles)
    return jnp.concatenate([front_half * cosine - back_half * sine_part, back_half * cosine + front_half * sine_part], axis=-1)

def reference(tokens, norm_gain, query_down, query_gain, latent_down, latent_gain, rope_down, query_up, key_up, value_up, glu_value, glu_gate, conv_taps, group_gain, head_proj, channel_proj):
    normed = rounded(rms_scale(tokens.astype(jnp.float32), norm_gain))
    positions = jnp.arange(LENGTH, dtype=jnp.int32)
    angles = angles_for(positions, ROPE)
    latent_query = rounded(rms_scale(jnp.dot(normed, query_down, preferred_element_type=jnp.float32), query_gain))
    query_all = jnp.dot(latent_query, query_up, preferred_element_type=jnp.float32).reshape(LENGTH, HEADS, NOPE + ROPE)
    query_plain = rounded(query_all[:, :, :NOPE])
    query_rope = rounded(rotate(query_all[:, :, NOPE:], angles[:, None, :]))
    absorbed = rounded(jnp.einsum('thd,rhd->htr', query_plain.astype(jnp.float32), key_up.astype(jnp.float32).reshape(KVR, HEADS, NOPE)))
    queries = jnp.concatenate([absorbed, jnp.transpose(query_rope, (1, 0, 2))], axis=-1).astype(jnp.float32)
    latent = rounded(rms_scale(jnp.dot(normed, latent_down, preferred_element_type=jnp.float32), latent_gain))
    rope_key = rounded(rotate(jnp.dot(normed, rope_down, preferred_element_type=jnp.float32), angles))
    keys = jnp.concatenate([latent, rope_key], axis=1).astype(jnp.float32)
    latent_wide = latent.astype(jnp.float32)
    score_scale = (NOPE + ROPE) ** (-0.5)
    block_count = LENGTH // TOK_DEV
    query_blocks = jnp.transpose(queries.reshape(HEADS, block_count, TOK_DEV, KVR + ROPE), (1, 0, 2, 3))

    def attend_block(query_block):
        scores = jnp.einsum('hqc,kc->hqk', query_block, keys) * score_scale
        row_max = lax.optimization_barrier(jnp.max(scores, axis=-1))
        weights = jnp.exp(scores - row_max[:, :, None])
        row_sum = lax.optimization_barrier(jnp.sum(weights, axis=-1))
        summed = jnp.einsum('hqk,kr->hqr', rounded(weights).astype(jnp.float32), latent_wide)
        return (rounded(summed / row_sum[:, :, None]), row_max + jnp.log(row_sum))
    attended, log_blocks = lax.map(attend_block, query_blocks)
    attended = jnp.transpose(attended, (1, 0, 2, 3)).reshape(HEADS, LENGTH, KVR)
    log_weight = jnp.transpose(log_blocks, (1, 0, 2)).reshape(HEADS, LENGTH)
    head_out = jnp.einsum('htr,rhv->thv', attended.astype(jnp.float32), value_up.astype(jnp.float32).reshape(KVR, HEADS, VDIM))
    head_out = rounded(head_out.reshape(LENGTH, HEADS * VDIM))
    value_in = jnp.dot(normed, glu_value, preferred_element_type=jnp.float32)
    gate_in = jnp.dot(normed, glu_gate, preferred_element_type=jnp.float32)
    gated_rows = rounded(value_in * jax.nn.sigmoid(gate_in))
    reach_rows = WIDTH // 2
    padded = jnp.pad(gated_rows.astype(jnp.float32), ((reach_rows, reach_rows), (0, 0)))
    filtered = padded[0:LENGTH] * conv_taps[0].astype(jnp.float32)
    for tap_index in range(1, WIDTH):
        filtered = filtered + padded[tap_index:tap_index + LENGTH] * conv_taps[tap_index].astype(jnp.float32)
    grouped = filtered.reshape(LENGTH, GROUPS, CH // GROUPS)
    centred = grouped - lax.optimization_barrier(jnp.mean(grouped, axis=-1, keepdims=True))
    spread = lax.optimization_barrier(jnp.mean(centred * centred, axis=-1, keepdims=True))
    normal_groups = (centred * lax.rsqrt(spread + norm_eps)).reshape(LENGTH, CH)
    conv_branch = rounded(jax.nn.silu(normal_groups * group_gain.astype(jnp.float32)))
    head_part = HEADS * VDIM // N_TP
    channel_part = CH // N_TP
    mixed_total = jnp.zeros((LENGTH, D), jnp.float32)
    for group_index in range(N_TP):
        head_lo = group_index * head_part
        chan_lo = group_index * channel_part
        partial_value = jnp.dot(head_out[:, head_lo:head_lo + head_part], head_proj[head_lo:head_lo + head_part], preferred_element_type=jnp.float32)
        partial_value = partial_value + jnp.dot(conv_branch[:, chan_lo:chan_lo + channel_part], channel_proj[chan_lo:chan_lo + channel_part], preferred_element_type=jnp.float32)
        mixed_total = mixed_total + rounded(partial_value).astype(jnp.float32)
    return (mixed_total.astype(jnp.bfloat16), log_weight)
```

```python
import functools
import math

import jax
import jax.numpy as jnp
import numpy as np
from jax import lax
from jax.experimental import pallas as pl
from jax.experimental.pallas import tpu as pltpu
from jax.sharding import PartitionSpec as P

NOPE = 128
ROPE = 64
VDIM = 128
KVR = 256
GROUP = 128
GRID_W = 64
EPS = 1e-06
BASE = 10000.0
HALO = 16
NX = 4
F32 = jnp.float32
BF16 = jnp.bfloat16
MESH = pl.DeviceIdType.MESH


def dot(a, b):
    return jnp.dot(a, b, preferred_element_type=F32)


def dot_t(a, b):
    return lax.dot_general(a, b, (((1,), (1,)), ((), ())), preferred_element_type=F32)


def rms(values, gain):
    inv = lax.rsqrt(jnp.mean(values * values, axis=-1, keepdims=True) + EPS)
    return values * inv * gain


def swap(v):
    half = v.shape[-1] // 2
    return jnp.concatenate([v[:, half:], v[:, :half]], axis=-1)


class Gather:
    def __init__(self, view, nz, ny, z, y, p_send, p_recv, r_send, r_recv):
        self.view, self.size, self.pos = view, (nz, ny), (z, y)
        self.p_send, self.p_recv, self.r_send, self.r_recv = p_send, p_recv, r_send, r_recv
        self.sent = []

    def device(self, axis, k):
        z, y = (k, self.pos[1]) if axis == 0 else (self.pos[0], k)
        return {"sp": z * self.size[1] + y}

    def first_copy(self, half, d, outgoing):
        axis = 1 - half
        n = self.size[axis]
        me = self.pos[axis]
        source = me if outgoing else lax.rem(me + n - d, n)
        z, y = (source, self.pos[1]) if axis == 0 else (self.pos[0], source)
        ref = self.view.at[z, y, half]
        return pltpu.make_async_remote_copy(
            src_ref=ref,
            dst_ref=ref,
            send_sem=self.p_send.at[half, d - 1],
            recv_sem=self.p_recv.at[half, d - 1],
            device_id=self.device(axis, lax.rem(me + d, n)),
            device_id_type=MESH,
        )

    def start_first(self):
        for half in (0, 1):
            for d in range(1, self.size[1 - half]):
                copy = self.first_copy(half, d, True)
                copy.start()
                self.sent.append(copy)

    def wait_first(self):
        for half in (0, 1):
            for d in range(1, self.size[1 - half]):
                self.first_copy(half, d, False).wait_recv()

    def block(self, half, k, part=None):
        n = self.size[1 - half]
        rows = slice(None) if part is None else pl.ds(part * (n // 2), n // 2)
        return self.view.at[k, rows, 0] if half == 0 else self.view.at[rows, k, 1]

    def steps(self, half):
        return self.size[half] // 2

    def ring_block(self, half, way, s, outgoing):
        n = self.size[half]
        back = s - 1 if outgoing else s
        sign = 1 - 2 * way
        k = lax.rem(self.pos[half] - sign * back + n, n)
        return self.block(half, k, way if s == n // 2 else None)

    def ring_copy(self, half, way, s, outgoing):
        n = self.size[half]
        ref = self.ring_block(half, way, s, outgoing)
        target = lax.rem(self.pos[half] + (1 - 2 * way) + n, n)
        return pltpu.make_async_remote_copy(
            src_ref=ref,
            dst_ref=ref,
            send_sem=self.r_send.at[half, way, s - 1],
            recv_sem=self.r_recv.at[half, way, s - 1],
            device_id=self.device(half, target),
            device_id_type=MESH,
        )

    def start_ring(self, s):
        for half in (0, 1):
            for way in (0, 1):
                copy = self.ring_copy(half, way, s, True)
                copy.start()
                self.sent.append(copy)

    def wait_ring(self, s):
        for half in (0, 1):
            for way in (0, 1):
                self.ring_copy(half, way, s, False).wait_recv()

    def finish(self):
        for copy in self.sent:
            copy.wait_send()


def kernel(
    nz,
    ny,
    tokens,
    norm_gain,
    down_shard,
    query_gain,
    latent_down,
    latent_gain,
    rope_down,
    query_up,
    key_up,
    value_up,
    conv_taps,
    group_gain,
    out_shard,
    inv_freq,
    out,
    log_weight,
    normed4,
    down_all,
    keys_all,
    out_all,
    ql_send,
    ql_recv,
    gated,
    wide,
    conv_send,
    conv_recv,
    queries,
    row_max,
    row_sum,
    acc,
    head_out,
    part_send,
    part_recv,
    local_sem,
    down_p_send,
    down_p_recv,
    down_r_send,
    down_r_recv,
    keys_p_send,
    keys_p_recv,
    keys_r_send,
    keys_r_recv,
    out_p_send,
    out_p_recv,
    out_r_send,
    out_r_recv,
    pair_send,
    pair_recv,
    pair0_send,
    pair0_recv,
    x_send,
    x_recv,
    xp_send,
    xp_recv,
    ql_ssem,
    ql_rsem,
    cv_ssem,
    cv_rsem,
    halo_ssem,
    halo_rsem,
    fin_sem,
):
    sp = lax.axis_index("sp")
    x = lax.axis_index("fs")
    c = lax.axis_index("tp")
    z, y = sp // ny, lax.rem(sp, ny)
    other = 1 - c
    count = tokens.shape[0]
    half_rows = count // 2
    heads = key_up.shape[1] // NOPE

    load_down = pltpu.make_async_copy(down_shard, down_all.at[z, y], local_sem.at[0])
    load_down.start()
    load_out = pltpu.make_async_copy(out_shard, out_all.at[z, y], local_sem.at[1])
    load_out.start()

    barrier = pltpu.get_barrier_semaphore()

    def greet(**where):
        pl.semaphore_signal(barrier, inc=1, device_id=where, device_id_type=MESH)

    for d in range(1, ny):
        greet(sp=z * ny + lax.rem(y + d, ny))
    for d in range(1, nz):
        greet(sp=lax.rem(z + d, nz) * ny + y)
    for d in range(1, NX):
        greet(fs=lax.rem(x + d, NX))
    greet(tp=other)
    has_low = sp > 0
    has_high = sp < nz * ny - 1

    @pl.when(has_low)
    def _():
        greet(sp=sp - 1)

    @pl.when(has_high)
    def _():
        greet(sp=sp + 1)

    gain = norm_gain[...].astype(F32)
    chunk = 32
    for k in range(count // chunk):
        rows = tokens[k * chunk : (k + 1) * chunk, :].astype(F32)
        value = rms(rows, gain).astype(BF16)
        which, first = divmod(k * chunk, half_rows)
        normed4[x, which, first : first + chunk, :] = value

    edges = has_low.astype(jnp.int32) + has_high.astype(jnp.int32)
    pl.semaphore_wait(barrier, (ny - 1) + (nz - 1) + (NX - 1) + 1 + edges)
    load_down.wait()
    load_out.wait()

    g_down = Gather(down_all, nz, ny, z, y, down_p_send, down_p_recv, down_r_send, down_r_recv)
    g_keys = Gather(keys_all.at[c], nz, ny, z, y, keys_p_send, keys_p_recv, keys_r_send, keys_r_recv)
    g_out = Gather(out_all, nz, ny, z, y, out_p_send, out_p_recv, out_r_send, out_r_recv)
    sent = []

    def send(src, dst, ssem, rsem, where):
        copy = pltpu.make_async_remote_copy(
            src_ref=src, dst_ref=dst, send_sem=ssem, recv_sem=rsem, device_id=where, device_id_type=MESH
        )
        copy.start()
        sent.append(copy)

    def arrived(dst, ssem, rsem, where):
        pltpu.make_async_remote_copy(
            src_ref=dst, dst_ref=dst, send_sem=ssem, recv_sem=rsem, device_id=where, device_id_type=MESH
        ).wait_recv()

    g_down.start_first()
    for way in (0, 1):
        mine = normed4.at[x, c]
        where = {"fs": lax.rem(x + (1 - 2 * way) + NX, NX)}
        send(mine, mine, x_send.at[way], x_recv.at[way], where)

    freq = inv_freq[...]
    at_row = lax.broadcasted_iota(jnp.int32, (count, ROPE), 0)
    lane = lax.broadcasted_iota(jnp.int32, (count, ROPE), 1)
    place = at_row + sp * count
    grid_row = (place // GRID_W).astype(F32)
    grid_col = lax.rem(place, GRID_W).astype(F32)
    angles = jnp.where(lax.rem(lane, ROPE // 2) < ROPE // 4, grid_row, grid_col) * freq
    cosine = jnp.cos(angles)
    sine = jnp.sin(angles) * jnp.where(lane < ROPE // 2, -1.0, 1.0)
    wide[0, 0:count, 0:ROPE] = cosine
    wide[1, 0:count, 0:ROPE] = sine

    own = normed4[x, c]
    latent = rms(dot(own, latent_down[...]), latent_gain[...].astype(F32))
    rope_key = dot(own, rope_down[...])
    first = pl.multiple_of(c * half_rows, half_rows)
    rope_key = rope_key * wide[0, pl.ds(first, half_rows), 0:ROPE] + swap(rope_key) * wide[
        1, pl.ds(first, half_rows), 0:ROPE
    ]
    quarter = half_rows // 2
    rope_pair = jnp.concatenate([rope_key[:quarter], rope_key[quarter:]], axis=1).astype(BF16)
    latent = latent.astype(BF16)
    for h in (0, 1):
        lo = h * (quarter // 2)
        hi = lo + quarter // 2
        keys_all[c, z, y, h, :, 0:KVR] = latent[lo:hi]
        keys_all[c, z, y, h, :, KVR : 2 * KVR] = latent[quarter + lo : quarter + hi]
        keys_all[c, z, y, h, :, 2 * KVR :] = rope_pair[lo:hi]

    g_keys.start_first()

    partner = {"tp": other}

    def pair_keys(half, way, s):
        block = g_keys.ring_block(half, way, s, False)
        send(block, block, pair_send.at[half, way, s - 1], pair_recv.at[half, way, s - 1], partner)

    g_down.wait_first()
    g_down.start_ring(1)
    g_keys.wait_first()
    g_keys.start_ring(1)
    own_block = (g_keys.block(0, z), g_keys.block(1, y))
    for half in (0, 1):
        send(own_block[half], own_block[half], pair0_send.at[half], pair0_recv.at[half], partner)

    turn = 1 - 2 * c
    far = lax.rem(x + 2, NX)
    for way in (0, 1):
        src = lax.rem(x - (1 - 2 * way) + NX, NX)
        piece = normed4.at[src, c]
        arrived(piece, x_send.at[way], x_recv.at[way], partner)
        send(piece, piece, xp_send.at[way], xp_recv.at[way], partner)
    onward = normed4.at[lax.rem(x - turn + NX, NX), c]
    send(onward, onward, x_send.at[2], x_recv.at[2], {"fs": lax.rem(x + turn + NX, NX)})

    last = nz // 2
    for s in range(1, last):
        g_down.wait_ring(s)
        g_down.start_ring(s + 1)
        g_keys.wait_ring(s)
        g_keys.start_ring(s + 1)
        for half in (0, 1):
            for way in (0, 1):
                pair_keys(half, way, s)
        if s == 1:
            piece = normed4.at[far, c]
            arrived(piece, x_send.at[2], x_recv.at[2], partner)
            send(piece, piece, xp_send.at[2], xp_recv.at[2], partner)

    g_out.start_first()

    for k in range(3):
        if k < 2:
            src = lax.rem(x - (1 - 2 * k) + NX, NX)
        else:
            src = far
        piece = normed4.at[src, other]
        arrived(piece, xp_send.at[k], xp_recv.at[k], partner)
    g_down.wait_ring(last)

    depth = tokens.shape[1]
    weights = down_all[...].reshape(depth, 3 * GROUP)
    for j in range(NX):
        rows = normed4[j].reshape(count, depth)
        product = dot(rows, weights)
        gate = product[:, GROUP : 2 * GROUP]
        gated[j, HALO : HALO + count, :] = (product[:, :GROUP] * jax.nn.sigmoid(gate)).astype(BF16)
        ql_send[j] = product[:, 2 * GROUP :]
    edge = jnp.zeros((NX, HALO, GROUP), BF16)

    low_src, high_src = gated.at[:, pl.ds(HALO, HALO)], gated.at[:, pl.ds(count, HALO)]
    low_dst, high_dst = gated.at[:, pl.ds(0, HALO)], gated.at[:, pl.ds(HALO + count, HALO)]

    def halo_copy(up):
        src, dst = (high_src, low_dst) if up else (low_src, high_dst)
        k = 0 if up else 1
        return pltpu.make_async_remote_copy(
            src_ref=src,
            dst_ref=dst,
            send_sem=halo_ssem.at[k],
            recv_sem=halo_rsem.at[k],
            device_id={"sp": sp + 1 if up else sp - 1},
            device_id_type=MESH,
        )

    @pl.when(has_high)
    def _():
        halo_copy(True).start()

    @pl.when(has_low)
    def _():
        halo_copy(False).start()

    def to_parts(src, dst, ssem, rsem):
        for d in range(1, NX):
            part = lax.rem(x + d, NX)
            send(src.at[part], dst.at[x], ssem.at[d - 1], rsem.at[d - 1], {"fs": part})

    def from_parts(dst, ssem, rsem):
        for d in range(1, NX):
            arrived(dst.at[lax.rem(x + NX - d, NX)], ssem.at[d - 1], rsem.at[d - 1], partner)

    to_parts(ql_send, ql_recv, ql_ssem, ql_rsem)
    ql_recv[x] = ql_send[x]

    @pl.when(jnp.logical_not(has_low))
    def _():
        gated[:, 0:HALO, :] = edge

    @pl.when(jnp.logical_not(has_high))
    def _():
        gated[:, HALO + count :, :] = edge

    g_keys.wait_ring(last)
    for half in (0, 1):
        for way in (0, 1):
            pair_keys(half, way, last)
    g_out.wait_first()
    g_out.start_ring(1)

    from_parts(ql_recv, ql_ssem, ql_rsem)
    latent_query = jnp.concatenate([ql_recv[k] for k in range(NX)], axis=1)
    latent_query = rms(latent_query, query_gain[...].astype(F32)).astype(BF16)
    query_all = dot(latent_query, query_up[...])
    cosine = wide[0, 0:count, 0:ROPE]
    sine = wide[1, 0:count, 0:ROPE]
    nothing = jnp.zeros((count, ROPE), F32)
    for h in range(heads):
        start = h * (NOPE + ROPE)
        plain = query_all[:, start : start + NOPE].astype(BF16)
        turned = query_all[:, start + NOPE : start + NOPE + ROPE]
        turned = turned * cosine + swap(turned) * sine
        absorbed = dot_t(plain, key_up[:, h * NOPE : (h + 1) * NOPE]).astype(BF16)
        rows = slice(h * count, (h + 1) * count)
        queries[0, rows, 0:KVR] = absorbed
        queries[1, rows, 0:KVR] = absorbed
        queries[0, rows, KVR:] = jnp.concatenate([turned, nothing], axis=1).astype(BF16)
        queries[1, rows, KVR:] = jnp.concatenate([nothing, turned], axis=1).astype(BF16)

    @pl.when(has_low)
    def _():
        halo_copy(True).wait_recv()

    @pl.when(has_high)
    def _():
        halo_copy(False).wait_recv()

    reach = conv_taps.shape[0] // 2
    columns = pl.ds(pl.multiple_of(x * GROUP, GROUP), GROUP)
    taps = conv_taps[:, columns].astype(F32)
    channel_gain = group_gain[x].astype(F32)
    for j in range(NX):
        wide[j, :, :] = gated[j].astype(F32)
        total = jnp.zeros((count, GROUP), F32)
        for t in range(2 * reach + 1):
            lo = HALO - reach + t
            total = total + wide[j, lo : lo + count, :] * taps[t : t + 1, :]
        centred = total - jnp.mean(total, axis=-1, keepdims=True)
        spread = jnp.mean(centred * centred, axis=-1, keepdims=True)
        conv_send[j] = jax.nn.silu(centred * lax.rsqrt(spread + EPS) * channel_gain).astype(BF16)
    to_parts(conv_send, conv_recv, cv_ssem, cv_rsem)
    conv_recv[x] = conv_send[x]

    other_keys = Gather(keys_all.at[other], nz, ny, z, y, keys_p_send, keys_p_recv, keys_r_send, keys_r_recv)
    for half in (0, 1):
        ref = other_keys.block(half, z if half == 0 else y)
        arrived(ref, pair0_send.at[half], pair0_recv.at[half], partner)
    for s in range(1, last + 1):
        for half in (0, 1):
            for way in (0, 1):
                ref = other_keys.ring_block(half, way, s, False)
                arrived(ref, pair_send.at[half, way, s - 1], pair_recv.at[half, way, s - 1], partner)

    scale = (NOPE + ROPE) ** (-0.5)
    factor = scale * math.log2(math.e)
    row_max[...] = jnp.full(row_max.shape, -1e30, F32)
    row_sum[...] = jnp.zeros(row_sum.shape, F32)
    acc[...] = jnp.zeros(acc.shape, F32)
    block_rows = ny * 2 * (quarter // 2)

    def attend(k, carry):
        pieces, values = [], []
        for core in (0, 1):
            block = keys_all[core, k].reshape(block_rows, 2 * KVR + 2 * ROPE)
            tail = block[:, 2 * KVR :]
            for low in (0, 1):
                value = block[:, low * KVR : (low + 1) * KVR]
                pieces.append(dot_t(queries[low], jnp.concatenate([value, tail], axis=1)))
                values.append(value)
        scores = jnp.concatenate(pieces, axis=1)
        before = row_max[...]
        now = jnp.maximum(before, jnp.max(scores, axis=1, keepdims=True))
        shrink = jnp.exp2((before - now) * factor)
        weights = jnp.exp2((scores - jnp.tile(now, (1, scores.shape[1] // 128))) * factor)
        row_sum[...] = row_sum[...] * shrink + jnp.sum(weights, axis=1, keepdims=True)
        row_max[...] = now
        added = dot(weights.astype(BF16), jnp.concatenate(values, axis=0))
        acc[...] = acc[...] * jnp.tile(shrink, (1, KVR // 128)) + added
        return carry

    groups = nz // last
    for s in range(1, last + 1):
        lax.fori_loop((s - 1) * groups, s * groups, attend, 0)
        g_out.wait_ring(s)
        if s < last:
            g_out.start_ring(s + 1)

    for h in range(heads):
        rows = slice(h * count, (h + 1) * count)
        attended = (acc[rows, :] / jnp.tile(row_sum[rows, :], (1, KVR // 128))).astype(BF16)
        head_out[:, h * VDIM : (h + 1) * VDIM] = dot(attended, value_up[:, h * VDIM : (h + 1) * VDIM]).astype(BF16)
        logs = row_max[rows, :] * scale + jnp.log(row_sum[rows, :])
        log_weight[h : h + 1, :] = jnp.transpose(logs)[0:1, :]

    from_parts(conv_recv, cv_ssem, cv_rsem)
    mixed = jnp.concatenate([head_out[...]] + [conv_recv[k] for k in range(NX)], axis=1)
    zs = nz // 2
    width = zs * ny * 2 * out_all.shape[3]

    def columns_of(core):
        return dot_t(mixed, out_all[pl.ds(core * zs, zs)].reshape(width, mixed.shape[1]))

    part_send[...] = columns_of(other).astype(BF16)
    send(part_send, part_recv, fin_sem.at[0], fin_sem.at[1], partner)
    kept = columns_of(c).astype(BF16).astype(F32)
    arrived(part_recv, fin_sem.at[0], fin_sem.at[1], partner)
    out[...] = (kept + part_recv[...].astype(F32)).astype(BF16)

    for copy in sent:
        copy.wait_send()
    for gather in (g_down, g_keys, g_out):
        gather.finish()

    @pl.when(has_high)
    def _():
        halo_copy(True).wait_send()

    @pl.when(has_low)
    def _():
        halo_copy(False).wait_send()


def per_device(
    nz,
    ny,
    tokens,
    norm_gain,
    query_down,
    query_gain,
    latent_down,
    latent_gain,
    rope_down,
    query_up,
    key_up,
    value_up,
    glu_value,
    glu_gate,
    conv_taps,
    group_gain,
    head_proj,
    channel_proj,
):
    count, depth = tokens.shape
    shard = query_down.shape[0]
    x = lax.axis_index("fs")
    heads = key_up.shape[1] // NOPE

    def plane(a):
        return lax.dynamic_slice_in_dim(a, x * GROUP, GROUP, 1)

    down_shard = jnp.concatenate([plane(glu_value), plane(glu_gate), plane(query_down)], axis=1)
    down_shard = down_shard.reshape(2, shard // 2, 3 * GROUP)
    out_cols = head_proj.shape[1]
    mixed = head_proj.shape[0] + channel_proj.shape[0]
    out_shard = jnp.concatenate([head_proj, channel_proj], axis=0).T.reshape(2, out_cols // 2, mixed)
    freq = (BASE ** (-np.arange(ROPE // 4, dtype=np.float64) / (ROPE // 4))).astype(np.float32)
    inv_freq = jnp.asarray(np.tile(freq, 4)[None, :])
    key_rows = count // 8
    key_width = 2 * KVR + 2 * ROPE
    hops = max(nz, ny) - 1
    last = max(nz, ny) // 2
    dma = pltpu.SemaphoreType.DMA
    gather_sems = [dma((2, hops)), dma((2, hops)), dma((2, 2, last)), dma((2, 2, last))]
    vmem = pl.BlockSpec(memory_space=pltpu.VMEM)
    hbm = pl.BlockSpec(memory_space=pltpu.HBM)
    operands = (
        (tokens, vmem),
        (norm_gain[None, :], vmem),
        (down_shard, hbm),
        (query_gain[None, :], vmem),
        (latent_down, vmem),
        (latent_gain[None, :], vmem),
        (rope_down, vmem),
        (query_up, vmem),
        (key_up, vmem),
        (value_up, vmem),
        (conv_taps, vmem),
        (group_gain.reshape(NX, 1, GROUP), vmem),
        (out_shard, hbm),
        (inv_freq, vmem),
    )
    half_cols = nz * ny * out_cols // 2
    return pl.pallas_call(
        functools.partial(kernel, nz, ny),
        out_shape=(
            jax.ShapeDtypeStruct((count, half_cols), BF16),
            jax.ShapeDtypeStruct((heads, count), F32),
        ),
        in_specs=[spec for _, spec in operands],
        out_specs=(vmem, vmem),
        scratch_shapes=[
            pltpu.VMEM((NX, 2, count // 2, depth), BF16),
            pltpu.VMEM((nz, ny, 2, shard // 2, 3 * GROUP), BF16),
            pltpu.VMEM((2, nz, ny, 2, key_rows, key_width), BF16),
            pltpu.VMEM((nz, ny, 2, out_cols // 2, mixed), BF16),
            pltpu.VMEM((NX, count, GROUP), F32),
            pltpu.VMEM((NX, count, GROUP), F32),
            pltpu.VMEM((NX, count + 2 * HALO, GROUP), BF16),
            pltpu.VMEM((NX, count + 2 * HALO, GROUP), F32),
            pltpu.VMEM((NX, count, GROUP), BF16),
            pltpu.VMEM((NX, count, GROUP), BF16),
            pltpu.VMEM((2, heads * count, KVR + 2 * ROPE), BF16),
            pltpu.VMEM((heads * count, 128), F32),
            pltpu.VMEM((heads * count, 128), F32),
            pltpu.VMEM((heads * count, KVR), F32),
            pltpu.VMEM((count, heads * VDIM), BF16),
            pltpu.VMEM((count, half_cols), BF16),
            pltpu.VMEM((count, half_cols), BF16),
            dma((2,)),
            *gather_sems,
            *gather_sems,
            *gather_sems,
            dma((2, 2, last)),
            dma((2, 2, last)),
            dma((2,)),
            dma((2,)),
            dma((3,)),
            dma((3,)),
            dma((3,)),
            dma((3,)),
            dma((3,)),
            dma((3,)),
            dma((3,)),
            dma((3,)),
            dma((2,)),
            dma((2,)),
            dma((2,)),
        ],
        compiler_params=pltpu.CompilerParams(
            collective_id=0, has_side_effects=True, vmem_limit_bytes=60 * 1024 * 1024
        ),
    )(*[value for value, _ in operands])


def solution(mesh):
    sp = mesh.shape["sp"]
    ny = math.isqrt(sp)
    nz = sp // ny
    in_specs = (
        P(("fs", "sp"), None),
        P(),
        P("sp", None),
        P(),
        P(),
        P(),
        P(),
        P(None, "tp"),
        P(None, "tp"),
        P(None, "tp"),
        P("sp", "tp"),
        P("sp", "tp"),
        P(None, "tp"),
        P("tp"),
        P("tp", "sp"),
        P("tp", "sp"),
    )
    out_specs = (P(("fs", "sp"), "tp"), P("tp", ("fs", "sp")))
    return jax.shard_map(
        functools.partial(per_device, nz, ny), mesh=mesh, in_specs=in_specs, out_specs=out_specs, check_vma=False
    )
```

```python
import functools
import math

import jax
import jax.numpy as jnp
import numpy as np
from jax import lax
from jax.experimental import pallas as pl
from jax.experimental.pallas import tpu as pltpu
from jax.sharding import PartitionSpec as P

NOPE = 128
ROPE = 64
VDIM = 128
KVR = 256
GROUP = 128
GRID_W = 64
EPS = 1e-06
BASE = 10000.0
HALO = 16
NX = 4
F32 = jnp.float32
BF16 = jnp.bfloat16
MESH = pl.DeviceIdType.MESH


def dot(a, b):
    return jnp.dot(a, b, preferred_element_type=F32)


def dot_t(a, b):
    return lax.dot_general(a, b, (((1,), (1,)), ((), ())), preferred_element_type=F32)


def rms(values, gain):
    inv = lax.rsqrt(jnp.mean(values * values, axis=-1, keepdims=True) + EPS)
    return values * inv * gain


def swap(v):
    half = v.shape[-1] // 2
    return jnp.concatenate([v[:, half:], v[:, :half]], axis=-1)


class Gather:
    def __init__(self, view, nz, ny, z, y, p_send, p_recv, r_send, r_recv):
        self.view, self.size, self.pos = view, (nz, ny), (z, y)
        self.p_send, self.p_recv, self.r_send, self.r_recv = p_send, p_recv, r_send, r_recv
        self.sent = []

    def device(self, axis, k):
        z, y = (k, self.pos[1]) if axis == 0 else (self.pos[0], k)
        return {"sp": z * self.size[1] + y}

    def first_copy(self, half, d, outgoing):
        axis = 1 - half
        n = self.size[axis]
        me = self.pos[axis]
        source = me if outgoing else lax.rem(me + n - d, n)
        z, y = (source, self.pos[1]) if axis == 0 else (self.pos[0], source)
        ref = self.view.at[z, y, half]
        return pltpu.make_async_remote_copy(
            src_ref=ref,
            dst_ref=ref,
            send_sem=self.p_send.at[half, d - 1],
            recv_sem=self.p_recv.at[half, d - 1],
            device_id=self.device(axis, lax.rem(me + d, n)),
            device_id_type=MESH,
        )

    def start_first(self):
        for half in (0, 1):
            for d in range(1, self.size[1 - half]):
                copy = self.first_copy(half, d, True)
                copy.start()
                self.sent.append(copy)

    def wait_first(self):
        for half in (0, 1):
            for d in range(1, self.size[1 - half]):
                self.first_copy(half, d, False).wait_recv()

    def block(self, half, k, part=None):
        n = self.size[1 - half]
        rows = slice(None) if part is None else pl.ds(part * (n // 2), n // 2)
        return self.view.at[k, rows, 0] if half == 0 else self.view.at[rows, k, 1]

    def steps(self, half):
        return self.size[half] // 2

    def ring_block(self, half, way, s, outgoing):
        n = self.size[half]
        back = s - 1 if outgoing else s
        sign = 1 - 2 * way
        k = lax.rem(self.pos[half] - sign * back + n, n)
        return self.block(half, k, way if s == n // 2 else None)

    def ring_copy(self, half, way, s, outgoing):
        n = self.size[half]
        ref = self.ring_block(half, way, s, outgoing)
        target = lax.rem(self.pos[half] + (1 - 2 * way) + n, n)
        return pltpu.make_async_remote_copy(
            src_ref=ref,
            dst_ref=ref,
            send_sem=self.r_send.at[half, way, s - 1],
            recv_sem=self.r_recv.at[half, way, s - 1],
            device_id=self.device(half, target),
            device_id_type=MESH,
        )

    def start_ring(self, s):
        for half in (0, 1):
            for way in (0, 1):
                copy = self.ring_copy(half, way, s, True)
                copy.start()
                self.sent.append(copy)

    def wait_ring(self, s):
        for half in (0, 1):
            for way in (0, 1):
                self.ring_copy(half, way, s, False).wait_recv()

    def direct_copy(self, half, d, outgoing):
        n = self.size[half]
        me = self.pos[half]
        ref = self.block(half, me if outgoing else lax.rem(me + n - d, n))
        return pltpu.make_async_remote_copy(
            src_ref=ref,
            dst_ref=ref,
            send_sem=self.r_send.at[half, d - 1],
            recv_sem=self.r_recv.at[half, d - 1],
            device_id=self.device(half, lax.rem(me + d, n)),
            device_id_type=MESH,
        )

    def start_direct(self):
        for half in (0, 1):
            for d in range(1, self.size[half]):
                copy = self.direct_copy(half, d, True)
                copy.start()
                self.sent.append(copy)

    def wait_direct(self):
        for half in (0, 1):
            for d in range(1, self.size[half]):
                self.direct_copy(half, d, False).wait_recv()

    def pass_on(self, s, each=None):
        for half in (0, 1):
            for way in (0, 1):
                self.ring_copy(half, way, s, False).wait_recv()
                if s < self.steps(half):
                    copy = self.ring_copy(half, way, s + 1, True)
                    copy.start()
                    self.sent.append(copy)
                if each is not None:
                    each(half, way, s)

    def finish(self):
        for copy in self.sent:
            copy.wait_send()


IN_HBM = (
    "tokens",
    "latent_down",
    "rope_down",
    "query_up",
    "key_up",
    "value_up",
    "conv_taps",
)
SHARDS = ("query_down", "glu_value", "glu_gate", "head_proj", "channel_proj")
GAINS = ("norm_gain", "query_gain", "latent_gain", "group_gain", "inv_freq")
SCRATCH = (
    "normed4",
    "query_w",
    "glu_w",
    "keys_all",
    "out_all",
    "ql_send",
    "ql_recv",
    "gated",
    "wide",
    "conv_send",
    "conv_recv",
    "queries",
    "row_max",
    "row_sum",
    "acc",
    "head_out",
    "part_send",
)
SEMS = (
    "load_sem",
    "shard_sem",
    "qw_ps",
    "qw_pr",
    "qw_rs",
    "qw_rr",
    "glu_ps",
    "glu_pr",
    "glu_rs",
    "glu_rr",
    "keys_ps",
    "keys_pr",
    "keys_rs",
    "keys_rr",
    "out_ps",
    "out_pr",
    "out_rs",
    "out_rr",
    "pair_send",
    "pair_recv",
    "pair0_send",
    "pair0_recv",
    "x_send",
    "x_recv",
    "xp_send",
    "xp_recv",
    "ql_ssem",
    "ql_rsem",
    "cv_ssem",
    "cv_rsem",
    "halo_ssem",
    "halo_rsem",
    "fin_sem",
)
OUTS = ("kept", "part_recv", "log_weight")


def kernel(nz, ny, *refs):
    names = IN_HBM + SHARDS + GAINS + OUTS + SCRATCH + tuple("v_" + n for n in IN_HBM) + SEMS
    r = dict(zip(names, refs, strict=True))
    body(nz, ny, r)


def body(nz, ny, r):
    sp = lax.axis_index("sp")
    x = lax.axis_index("fs")
    c = lax.axis_index("tp")
    z, y = sp // ny, lax.rem(sp, ny)
    other = 1 - c
    tokens, latent_down, rope_down = r["v_tokens"], r["v_latent_down"], r["v_rope_down"]
    query_up, key_up, value_up, conv_taps = (r["v_" + n] for n in ("query_up", "key_up", "value_up", "conv_taps"))
    normed4, keys_all, out_all, gated, wide = (r[n] for n in ("normed4", "keys_all", "out_all", "gated", "wide"))
    query_w, glu_w, queries = r["query_w"], r["glu_w"], r["queries"]
    row_max, row_sum, acc = r["row_max"], r["row_sum"], r["acc"]
    count, depth = tokens.shape
    half_rows = count // 2
    heads = key_up.shape[1] // NOPE
    partner = {"tp": other}

    barrier = pltpu.get_barrier_semaphore()

    def greet(**where):
        pl.semaphore_signal(barrier, inc=1, device_id=where, device_id_type=MESH)

    for d in range(1, ny):
        greet(sp=z * ny + lax.rem(y + d, ny))
    for d in range(1, nz):
        greet(sp=lax.rem(z + d, nz) * ny + y)
    for d in range(1, NX):
        greet(fs=lax.rem(x + d, NX))
    greet(tp=other)
    has_low = sp > 0
    has_high = sp < nz * ny - 1

    @pl.when(has_low)
    def _():
        greet(sp=sp - 1)

    @pl.when(has_high)
    def _():
        greet(sp=sp + 1)

    loads = {}
    for k, name in enumerate(IN_HBM):
        loads[name] = pltpu.make_async_copy(r[name], r["v_" + name], r["load_sem"].at[k])
        loads[name].start()
        if k == 0:
            columns = pl.ds(pl.multiple_of(x * GROUP, GROUP), GROUP)
            slot = (z, y)
            wide_out = r["head_proj"].shape[-1]
            shards = (
                (r["query_down"].at[:, :, columns], query_w.at[slot]),
                (r["glu_value"].at[:, :, columns], glu_w.at[z, y, :, :, pl.ds(0, GROUP)]),
                (r["glu_gate"].at[:, :, columns], glu_w.at[z, y, :, :, pl.ds(GROUP, GROUP)]),
                (r["head_proj"], out_all.at[z, y, :, :, pl.ds(0, wide_out)]),
                (r["channel_proj"], out_all.at[z, y, :, :, pl.ds(wide_out, wide_out)]),
            )
            shards = [pltpu.make_async_copy(a, b, r["shard_sem"].at[i]) for i, (a, b) in enumerate(shards)]
            for copy in shards:
                copy.start()

    g_query = Gather(query_w, nz, ny, z, y, r["qw_ps"], r["qw_pr"], r["qw_rs"], r["qw_rr"])
    g_glu = Gather(glu_w, nz, ny, z, y, r["glu_ps"], r["glu_pr"], r["glu_rs"], r["glu_rr"])
    keys_sems = (r["keys_ps"], r["keys_pr"], r["keys_rs"], r["keys_rr"])
    g_keys = Gather(keys_all.at[c], nz, ny, z, y, *keys_sems)
    other_keys = Gather(keys_all.at[other], nz, ny, z, y, *keys_sems)
    g_out = Gather(out_all, nz, ny, z, y, r["out_ps"], r["out_pr"], r["out_rs"], r["out_rr"])
    sent = []

    def send(src, dst, ssem, rsem, where):
        copy = pltpu.make_async_remote_copy(
            src_ref=src, dst_ref=dst, send_sem=ssem, recv_sem=rsem, device_id=where, device_id_type=MESH
        )
        copy.start()
        sent.append(copy)

    def arrived(dst, ssem, rsem):
        pltpu.make_async_remote_copy(
            src_ref=dst, dst_ref=dst, send_sem=ssem, recv_sem=rsem, device_id=partner, device_id_type=MESH
        ).wait_recv()

    at_row = lax.broadcasted_iota(jnp.int32, (count, ROPE), 0)
    lane = lax.broadcasted_iota(jnp.int32, (count, ROPE), 1)
    place = at_row + sp * count
    grid_row = (place // GRID_W).astype(F32)
    grid_col = lax.rem(place, GRID_W).astype(F32)
    angles = jnp.where(lax.rem(lane, ROPE // 2) < ROPE // 4, grid_row, grid_col) * r["inv_freq"][...]
    wide[0, 0:count, 0:ROPE] = jnp.cos(angles)
    wide[1, 0:count, 0:ROPE] = jnp.sin(angles) * jnp.where(lane < ROPE // 2, -1.0, 1.0)

    loads["tokens"].wait()
    gain = r["norm_gain"][...].astype(F32)[None, :]
    chunk = 32
    for k in range(count // chunk):
        rows = tokens[k * chunk : (k + 1) * chunk, :].astype(F32)
        value = rms(rows, gain).astype(BF16)
        which, first = divmod(k * chunk, half_rows)
        normed4[x, which, first : first + chunk, :] = value

    loads["latent_down"].wait()
    loads["rope_down"].wait()
    own = normed4[x, c]
    latent = rms(dot(own, latent_down[...]), r["latent_gain"][...].astype(F32)[None, :]).astype(BF16)
    rope_key = dot_t(own, rope_down[...])
    first = pl.multiple_of(c * half_rows, half_rows)
    rope_key = rope_key * wide[0, pl.ds(first, half_rows), 0:ROPE] + swap(rope_key) * wide[
        1, pl.ds(first, half_rows), 0:ROPE
    ]
    quarter = half_rows // 2
    rope_pair = jnp.concatenate([rope_key[:quarter], rope_key[quarter:]], axis=1).astype(BF16)
    for h in (0, 1):
        lo = h * (quarter // 2)
        hi = lo + quarter // 2
        keys_all[c, z, y, h, :, 0:KVR] = latent[lo:hi]
        keys_all[c, z, y, h, :, KVR : 2 * KVR] = latent[quarter + lo : quarter + hi]
        keys_all[c, z, y, h, :, 2 * KVR :] = rope_pair[lo:hi]

    for copy in shards:
        copy.wait()
    edges = has_low.astype(jnp.int32) + has_high.astype(jnp.int32)
    pl.semaphore_wait(barrier, (ny - 1) + (nz - 1) + (NX - 1) + 1 + edges)

    g_query.start_first()
    for way in (0, 1):
        mine = normed4.at[x, c]
        where = {"fs": lax.rem(x + (1 - 2 * way) + NX, NX)}
        send(mine, mine, r["x_send"].at[way], r["x_recv"].at[way], where)
    g_keys.start_first()
    g_glu.start_first()
    g_out.start_first()
    for name in IN_HBM[3:]:
        loads[name].wait()

    def pair_keys(half, way, s):
        block = g_keys.ring_block(half, way, s, False)
        sems = r["pair_send"].at[half, way, s - 1], r["pair_recv"].at[half, way, s - 1]
        send(block, block, *sems, partner)

    g_query.wait_first()
    g_query.start_direct()

    turn = 1 - 2 * c
    far = lax.rem(x + 2, NX)
    for way in (0, 1):
        src = lax.rem(x - (1 - 2 * way) + NX, NX)
        piece = normed4.at[src, c]
        arrived(piece, r["x_send"].at[way], r["x_recv"].at[way])
        send(piece, piece, r["xp_send"].at[way], r["xp_recv"].at[way], partner)
    onward = normed4.at[lax.rem(x - turn + NX, NX), c]
    send(onward, onward, r["x_send"].at[2], r["x_recv"].at[2], {"fs": lax.rem(x + turn + NX, NX)})

    last = nz // 2
    g_keys.wait_first()
    g_keys.start_ring(1)
    own_block = (g_keys.block(0, z), g_keys.block(1, y))
    for half in (0, 1):
        send(own_block[half], own_block[half], r["pair0_send"].at[half], r["pair0_recv"].at[half], partner)
    g_glu.wait_first()
    g_glu.start_ring(1)
    g_out.wait_first()
    g_out.start_ring(1)

    g_keys.pass_on(1, pair_keys)
    g_glu.pass_on(1)
    piece = normed4.at[far, c]
    arrived(piece, r["x_send"].at[2], r["x_recv"].at[2])
    send(piece, piece, r["xp_send"].at[2], r["xp_recv"].at[2], partner)
    g_out.pass_on(1)

    def to_parts(src, dst, ssem, rsem):
        for d in range(1, NX):
            part = lax.rem(x + d, NX)
            send(src.at[part], dst.at[x], ssem.at[d - 1], rsem.at[d - 1], {"fs": part})

    def from_parts(dst, ssem, rsem):
        for d in range(1, NX):
            arrived(dst.at[lax.rem(x + NX - d, NX)], ssem.at[d - 1], rsem.at[d - 1])

    g_query.wait_direct()
    for k in range(3):
        src = far if k == 2 else lax.rem(x - (1 - 2 * k) + NX, NX)
        arrived(normed4.at[src, other], r["xp_send"].at[k], r["xp_recv"].at[k])
    ql_send, ql_recv = r["ql_send"], r["ql_recv"]
    everyone = normed4[...].reshape(NX * count, depth)
    ql_send[...] = dot(everyone, query_w[...].reshape(depth, GROUP)).reshape(NX, count, GROUP)
    to_parts(ql_send, ql_recv, r["ql_ssem"], r["ql_rsem"])
    ql_recv[x] = ql_send[x]

    g_keys.pass_on(2, pair_keys)
    g_glu.pass_on(2)
    g_out.pass_on(2)

    from_parts(ql_recv, r["ql_ssem"], r["ql_rsem"])
    latent_query = jnp.concatenate([ql_recv[k] for k in range(NX)], axis=1)
    latent_query = rms(latent_query, r["query_gain"][...].astype(F32)[None, :]).astype(BF16)
    query_all = dot(latent_query, query_up[...])
    cosine = wide[0, 0:count, 0:ROPE]
    sine = wide[1, 0:count, 0:ROPE]
    nothing = jnp.zeros((count, ROPE), F32)
    for h in range(heads):
        start = h * (NOPE + ROPE)
        plain = query_all[:, start : start + NOPE].astype(BF16)
        turned = query_all[:, start + NOPE : start + NOPE + ROPE]
        turned = turned * cosine + swap(turned) * sine
        absorbed = dot_t(plain, key_up[:, h * NOPE : (h + 1) * NOPE]).astype(BF16)
        rows = slice(h * count, (h + 1) * count)
        queries[0, rows, 0:KVR] = absorbed
        queries[1, rows, 0:KVR] = absorbed
        queries[0, rows, KVR:] = jnp.concatenate([turned, nothing], axis=1).astype(BF16)
        queries[1, rows, KVR:] = jnp.concatenate([nothing, turned], axis=1).astype(BF16)

    scale = (NOPE + ROPE) ** (-0.5)
    factor = scale * math.log2(math.e)
    row_max[...] = jnp.full(row_max.shape, -1e30, F32)
    row_sum[...] = jnp.zeros(row_sum.shape, F32)
    acc[...] = jnp.zeros(acc.shape, F32)
    lines = quarter // 2

    def attend(k, carry):
        odd = lax.rem(k, 2)
        step = odd * (lax.div(k, 2) + 1) - (1 - odd) * lax.div(k, 2)
        row = lax.rem(z + step + nz, nz)
        column = lax.rem(y + step + ny, ny)
        pieces, values = [], []
        for core in (0, 1):
            upper = keys_all[core, row, :, 0].reshape(ny * lines, 2 * KVR + 2 * ROPE)
            lower = keys_all[core, :, column, 1].reshape(nz * lines, 2 * KVR + 2 * ROPE)
            block = jnp.concatenate([upper, lower], axis=0)
            tail = block[:, 2 * KVR :]
            for low in (0, 1):
                value = block[:, low * KVR : (low + 1) * KVR]
                pieces.append(dot_t(queries[low], jnp.concatenate([value, tail], axis=1)))
                values.append(value)
        scores = jnp.concatenate(pieces, axis=1)
        before = row_max[...]
        now = jnp.maximum(before, jnp.max(scores, axis=1, keepdims=True))
        shrink = jnp.exp2((before - now) * factor)
        weights = jnp.exp2((scores - jnp.tile(now, (1, scores.shape[1] // 128))) * factor)
        row_sum[...] = row_sum[...] * shrink + jnp.sum(weights, axis=1, keepdims=True)
        row_max[...] = now
        added = dot(weights.astype(BF16), jnp.concatenate(values, axis=0))
        acc[...] = acc[...] * jnp.tile(shrink, (1, KVR // 128)) + added
        return carry

    def pair_arrived(s):
        for half in (0, 1):
            for way in (0, 1):
                ref = other_keys.ring_block(half, way, s, False)
                arrived(ref, r["pair_send"].at[half, way, s - 1], r["pair_recv"].at[half, way, s - 1])

    g_keys.pass_on(3, pair_keys)
    g_glu.pass_on(3)
    for half in (0, 1):
        ref = other_keys.block(half, z if half == 0 else y)
        arrived(ref, r["pair0_send"].at[half], r["pair0_recv"].at[half])
    pair_arrived(1)
    lax.fori_loop(0, 3, attend, 0)
    g_out.pass_on(3)
    pair_arrived(2)
    lax.fori_loop(3, 5, attend, 0)
    g_keys.pass_on(4, pair_keys)
    pair_arrived(3)
    lax.fori_loop(5, 7, attend, 0)

    g_glu.pass_on(4)
    glu_weights = glu_w[...].reshape(depth, 2 * GROUP)
    for j in range(NX):
        product = dot(normed4[j].reshape(count, depth), glu_weights)
        gated[j, HALO : HALO + count, :] = (product[:, :GROUP] * jax.nn.sigmoid(product[:, GROUP:])).astype(BF16)

    low_src, high_src = gated.at[:, pl.ds(HALO, HALO)], gated.at[:, pl.ds(count, HALO)]
    low_dst, high_dst = gated.at[:, pl.ds(0, HALO)], gated.at[:, pl.ds(HALO + count, HALO)]

    def halo_copy(up):
        src, dst = (high_src, low_dst) if up else (low_src, high_dst)
        k = 0 if up else 1
        return pltpu.make_async_remote_copy(
            src_ref=src,
            dst_ref=dst,
            send_sem=r["halo_ssem"].at[k],
            recv_sem=r["halo_rsem"].at[k],
            device_id={"sp": sp + 1 if up else sp - 1},
            device_id_type=MESH,
        )

    @pl.when(has_high)
    def _():
        halo_copy(True).start()

    @pl.when(has_low)
    def _():
        halo_copy(False).start()

    edge = jnp.zeros((NX, HALO, GROUP), BF16)

    @pl.when(jnp.logical_not(has_low))
    def _():
        gated[:, 0:HALO, :] = edge

    @pl.when(jnp.logical_not(has_high))
    def _():
        gated[:, HALO + count :, :] = edge

    pair_arrived(4)
    lax.fori_loop(7, 8, attend, 0)

    @pl.when(has_low)
    def _():
        halo_copy(True).wait_recv()

    @pl.when(has_high)
    def _():
        halo_copy(False).wait_recv()

    conv_send, conv_recv = r["conv_send"], r["conv_recv"]
    reach = conv_taps.shape[0] // 2
    taps = conv_taps[:, columns].astype(F32)
    gains = r["group_gain"][...].astype(F32)[None, :]
    channel_gain = gains[:, :GROUP]
    for k in range(1, NX):
        channel_gain = jnp.where(x == k, gains[:, k * GROUP : (k + 1) * GROUP], channel_gain)
    for j in range(NX):
        wide[j, :, :] = gated[j].astype(F32)
        total = jnp.zeros((count, GROUP), F32)
        for t in range(2 * reach + 1):
            lo = HALO - reach + t
            total = total + wide[j, lo : lo + count, :] * taps[t : t + 1, :]
        centred = total - jnp.mean(total, axis=-1, keepdims=True)
        spread = jnp.mean(centred * centred, axis=-1, keepdims=True)
        conv_send[j] = jax.nn.silu(centred * lax.rsqrt(spread + EPS) * channel_gain).astype(BF16)
    to_parts(conv_send, conv_recv, r["cv_ssem"], r["cv_rsem"])
    conv_recv[x] = conv_send[x]

    head_out, log_weight = r["head_out"], r["log_weight"]
    for h in range(heads):
        rows = slice(h * count, (h + 1) * count)
        attended = (acc[rows, :] / jnp.tile(row_sum[rows, :], (1, KVR // 128))).astype(BF16)
        head_out[:, h * VDIM : (h + 1) * VDIM] = dot(attended, value_up[:, h * VDIM : (h + 1) * VDIM]).astype(BF16)
        logs = row_max[rows, :] * scale + jnp.log(row_sum[rows, :])
        log_weight[h : h + 1, :] = jnp.transpose(logs)[0:1, :]

    from_parts(conv_recv, r["cv_ssem"], r["cv_rsem"])
    mixed = jnp.concatenate([head_out[...]] + [conv_recv[k] for k in range(NX)], axis=1)
    zs = nz // 2
    width = zs * ny * 2 * out_all.shape[3]
    part_send, part_recv = r["part_send"], r["part_recv"]
    g_out.pass_on(4)

    def columns_of(core):
        return dot_t(mixed, out_all[pl.ds(core * zs, zs)].reshape(width, mixed.shape[1])).astype(BF16)

    part_send[...] = columns_of(other)
    send(part_send, part_recv, r["fin_sem"].at[0], r["fin_sem"].at[1], partner)
    r["kept"][...] = columns_of(c)
    arrived(part_recv, r["fin_sem"].at[0], r["fin_sem"].at[1])

    for copy in sent:
        copy.wait_send()
    for gather in (g_query, g_glu, g_keys, g_out):
        gather.finish()

    @pl.when(has_high)
    def _():
        halo_copy(True).wait_send()

    @pl.when(has_low)
    def _():
        halo_copy(False).wait_send()


def per_device(
    nz,
    ny,
    tokens,
    norm_gain,
    query_down,
    query_gain,
    latent_down,
    latent_gain,
    rope_down,
    query_up,
    key_up,
    value_up,
    glu_value,
    glu_gate,
    conv_taps,
    group_gain,
    head_proj,
    channel_proj,
):
    count, depth = tokens.shape
    heads = key_up.shape[1] // NOPE

    def halves(a):
        return a.reshape(2, a.shape[0] // 2, a.shape[1])

    freq = (BASE ** (-np.arange(ROPE // 4, dtype=np.float64) / (ROPE // 4))).astype(np.float32)
    given = {
        "tokens": tokens,
        "latent_down": latent_down,
        "rope_down": rope_down.T,
        "query_up": query_up,
        "key_up": key_up,
        "value_up": value_up,
        "conv_taps": conv_taps,
        "query_down": halves(query_down),
        "glu_value": halves(glu_value),
        "glu_gate": halves(glu_gate),
        "head_proj": halves(head_proj.T),
        "channel_proj": halves(channel_proj.T),
        "norm_gain": norm_gain,
        "query_gain": query_gain,
        "latent_gain": latent_gain,
        "group_gain": group_gain,
        "inv_freq": jnp.asarray(np.tile(freq, 4)[None, :]),
    }
    shard = query_down.shape[0] // 2
    out_cols = head_proj.shape[1]
    mixed = head_proj.shape[0] + channel_proj.shape[0]
    half_cols = nz * ny * out_cols // 2
    hops = max(nz, ny) - 1
    last = max(nz, ny) // 2
    dma = pltpu.SemaphoreType.DMA
    vmem = pl.BlockSpec(memory_space=pltpu.VMEM)
    hbm = pl.BlockSpec(memory_space=pltpu.HBM)

    def buf(*shape, dtype=BF16):
        return pltpu.VMEM(shape, dtype)

    ring = [dma((2, hops)), dma((2, hops)), dma((2, 2, last)), dma((2, 2, last))]
    scratch = [
        buf(NX, 2, count // 2, depth),
        buf(nz, ny, 2, shard, GROUP),
        buf(nz, ny, 2, shard, 2 * GROUP),
        buf(2, nz, ny, 2, count // 8, 2 * KVR + 2 * ROPE),
        buf(nz, ny, 2, out_cols // 2, mixed),
        buf(NX, count, GROUP, dtype=F32),
        buf(NX, count, GROUP, dtype=F32),
        buf(NX, count + 2 * HALO, GROUP),
        buf(NX, count + 2 * HALO, GROUP, dtype=F32),
        buf(NX, count, GROUP),
        buf(NX, count, GROUP),
        buf(2, heads * count, KVR + 2 * ROPE),
        buf(heads * count, 128, dtype=F32),
        buf(heads * count, 128, dtype=F32),
        buf(heads * count, KVR, dtype=F32),
        buf(count, heads * VDIM),
        buf(count, half_cols),
        *[buf(*given[name].shape) for name in IN_HBM],
        dma((len(IN_HBM),)),
        dma((len(SHARDS),)),
        *[dma((2, hops))] * 4,
        *ring,
        *ring,
        *ring,
        dma((2, 2, last)),
        dma((2, 2, last)),
        dma((2,)),
        dma((2,)),
        *[dma((3,))] * 8,
        *[dma((2,))] * 3,
    ]
    kept, came, log_weight = pl.pallas_call(
        functools.partial(kernel, nz, ny),
        out_shape=(
            jax.ShapeDtypeStruct((count, half_cols), BF16),
            jax.ShapeDtypeStruct((count, half_cols), BF16),
            jax.ShapeDtypeStruct((heads, count), F32),
        ),
        in_specs=[hbm] * (len(IN_HBM) + len(SHARDS)) + [vmem] * len(GAINS),
        out_specs=(vmem, vmem, vmem),
        scratch_shapes=scratch,
        compiler_params=pltpu.CompilerParams(
            collective_id=0, has_side_effects=True, vmem_limit_bytes=60 * 1024 * 1024
        ),
    )(*[given[name] for name in IN_HBM + SHARDS + GAINS])
    return (kept.astype(F32) + came.astype(F32)).astype(BF16), log_weight


def solution(mesh):
    sp = mesh.shape["sp"]
    ny = math.isqrt(sp)
    nz = sp // ny
    in_specs = (
        P(("fs", "sp"), None),
        P(),
        P("sp", None),
        P(),
        P(),
        P(),
        P(),
        P(None, "tp"),
        P(None, "tp"),
        P(None, "tp"),
        P("sp", "tp"),
        P("sp", "tp"),
        P(None, "tp"),
        P("tp"),
        P("tp", "sp"),
        P("tp", "sp"),
    )
    out_specs = (P(("fs", "sp"), "tp"), P("tp", ("fs", "sp")))
    return jax.shard_map(
        functools.partial(per_device, nz, ny), mesh=mesh, in_specs=in_specs, out_specs=out_specs, check_vma=False
    )
```

```python
import functools
import math

import jax
import jax.numpy as jnp
import numpy as np
from jax import lax
from jax.experimental import pallas as pl
from jax.experimental.pallas import tpu as pltpu
from jax.sharding import PartitionSpec as P

NOPE = 128
ROPE = 64
VDIM = 128
KVR = 256
GROUP = 128
GRID_W = 64
EPS = 1e-06
BASE = 10000.0
HALO = 16
NX = 4
F32 = jnp.float32
BF16 = jnp.bfloat16
MESH = pl.DeviceIdType.MESH


def dot(a, b):
    return jnp.dot(a, b, preferred_element_type=F32)


def dot_t(a, b):
    return lax.dot_general(a, b, (((1,), (1,)), ((), ())), preferred_element_type=F32)


def rms(values, gain):
    inv = lax.rsqrt(jnp.mean(values * values, axis=-1, keepdims=True) + EPS)
    return values * inv * gain


def swap(v):
    half = v.shape[-1] // 2
    return jnp.concatenate([v[:, half:], v[:, :half]], axis=-1)


class Gather:
    def __init__(self, view, nz, ny, z, y, p_send, p_recv, r_send, r_recv):
        self.view, self.size, self.pos = view, (nz, ny), (z, y)
        self.p_send, self.p_recv, self.r_send, self.r_recv = p_send, p_recv, r_send, r_recv
        self.sent = []

    def device(self, axis, k):
        z, y = (k, self.pos[1]) if axis == 0 else (self.pos[0], k)
        return {"sp": z * self.size[1] + y}

    def first_copy(self, half, d, outgoing):
        axis = 1 - half
        n = self.size[axis]
        me = self.pos[axis]
        source = me if outgoing else lax.rem(me + n - d, n)
        z, y = (source, self.pos[1]) if axis == 0 else (self.pos[0], source)
        ref = self.view.at[z, y, half]
        return pltpu.make_async_remote_copy(
            src_ref=ref,
            dst_ref=ref,
            send_sem=self.p_send.at[half, d - 1],
            recv_sem=self.p_recv.at[half, d - 1],
            device_id=self.device(axis, lax.rem(me + d, n)),
            device_id_type=MESH,
        )

    def start_first(self):
        for half in (0, 1):
            for d in range(1, self.size[1 - half]):
                copy = self.first_copy(half, d, True)
                copy.start()
                self.sent.append(copy)

    def wait_first(self):
        for half in (0, 1):
            for d in range(1, self.size[1 - half]):
                self.first_copy(half, d, False).wait_recv()

    def block(self, half, k, part=None):
        n = self.size[1 - half]
        rows = slice(None) if part is None else pl.ds(part * (n // 2), n // 2)
        return self.view.at[k, rows, 0] if half == 0 else self.view.at[rows, k, 1]

    def steps(self, half):
        return self.size[half] // 2

    def ring_block(self, half, way, s, outgoing):
        n = self.size[half]
        back = s - 1 if outgoing else s
        sign = 1 - 2 * way
        k = lax.rem(self.pos[half] - sign * back + n, n)
        return self.block(half, k, way if s == n // 2 else None)

    def ring_copy(self, half, way, s, outgoing):
        n = self.size[half]
        ref = self.ring_block(half, way, s, outgoing)
        target = lax.rem(self.pos[half] + (1 - 2 * way) + n, n)
        return pltpu.make_async_remote_copy(
            src_ref=ref,
            dst_ref=ref,
            send_sem=self.r_send.at[half, way, s - 1],
            recv_sem=self.r_recv.at[half, way, s - 1],
            device_id=self.device(half, target),
            device_id_type=MESH,
        )

    def start_ring(self, s):
        for half in (0, 1):
            for way in (0, 1):
                copy = self.ring_copy(half, way, s, True)
                copy.start()
                self.sent.append(copy)

    def wait_ring(self, s):
        for half in (0, 1):
            for way in (0, 1):
                self.ring_copy(half, way, s, False).wait_recv()

    def pass_on(self, s, each=None):
        for half in (0, 1):
            for way in (0, 1):
                self.ring_copy(half, way, s, False).wait_recv()
                if s < self.steps(half):
                    copy = self.ring_copy(half, way, s + 1, True)
                    copy.start()
                    self.sent.append(copy)
                if each is not None:
                    each(half, way, s)

    def finish(self):
        for copy in self.sent:
            copy.wait_send()


def kernel(
    nz,
    ny,
    tokens_hbm,
    latent_down_hbm,
    rope_down_hbm,
    query_up_hbm,
    key_up_hbm,
    value_up_hbm,
    conv_taps_hbm,
    query_down,
    glu_value,
    glu_gate,
    head_proj,
    channel_proj,
    norm_gain,
    query_gain,
    latent_gain,
    group_gain,
    inv_freq,
    kept,
    part_recv,
    log_weight,
    normed4,
    query_w,
    glu_w,
    ch_all,
    keys_all,
    out_all,
    ql_send,
    ql_recv,
    gated,
    wide,
    conv_send,
    conv_recv,
    queries,
    row_max,
    row_sum,
    acc,
    head_out,
    part_send,
    tokens,
    latent_down,
    rope_down,
    query_up,
    key_up,
    value_up,
    conv_taps,
    load_sem,
    shard_sem,
    qw_ps,
    qw_pr,
    qw_rs,
    qw_rr,
    glu_ps,
    glu_pr,
    glu_rs,
    glu_rr,
    ch_ps,
    ch_pr,
    ch_rs,
    ch_rr,
    keys_ps,
    keys_pr,
    keys_rs,
    keys_rr,
    out_ps,
    out_pr,
    out_rs,
    out_rr,
    qp_send,
    qp_recv,
    chx_send,
    chx_recv,
    chx0_send,
    chx0_recv,
    chr_send,
    chr_recv,
    chr0_send,
    chr0_recv,
    pair_send,
    pair_recv,
    pair0_send,
    pair0_recv,
    x_send,
    x_recv,
    xp_send,
    xp_recv,
    ql_ssem,
    ql_rsem,
    cv_ssem,
    cv_rsem,
    halo_ssem,
    halo_rsem,
    fin_sem,
):
    sp = lax.axis_index("sp")
    x = lax.axis_index("fs")
    c = lax.axis_index("tp")
    z, y = sp // ny, lax.rem(sp, ny)
    other = 1 - c
    count, depth = tokens.shape
    half_rows = count // 2
    heads = key_up.shape[1] // NOPE
    partner = {"tp": other}
    turn = 1 - 2 * c
    behind, ahead, far = lax.rem(x - turn + NX, NX), lax.rem(x + turn + NX, NX), lax.rem(x + 2, NX)

    barrier = pltpu.get_barrier_semaphore()

    def greet(**where):
        pl.semaphore_signal(barrier, inc=1, device_id=where, device_id_type=MESH)

    for d in range(1, ny):
        greet(sp=z * ny + lax.rem(y + d, ny))
    for d in range(1, nz):
        greet(sp=lax.rem(z + d, nz) * ny + y)
    for d in range(1, NX):
        greet(fs=lax.rem(x + d, NX))
    greet(tp=other)
    has_low = sp > 0
    has_high = sp < nz * ny - 1

    @pl.when(has_low)
    def _():
        greet(sp=sp - 1)

    @pl.when(has_high)
    def _():
        greet(sp=sp + 1)

    first_core = c == 0
    a_pos, b_pos = jnp.where(first_core, z, y), jnp.where(first_core, y, z)
    columns = pl.ds(pl.multiple_of(x * GROUP, GROUP), GROUP)
    slots = (
        (query_down.at[c, :, columns], query_w.at[c, a_pos, b_pos]),
        (glu_value.at[:, :, columns], glu_w.at[z, y, :, :, pl.ds(0, GROUP)]),
        (glu_gate.at[:, :, columns], glu_w.at[z, y, :, :, pl.ds(GROUP, GROUP)]),
        (channel_proj.at[:, :, columns], ch_all.at[x, z, y]),
        (head_proj, out_all.at[z, y]),
    )
    wanted = (
        (tokens_hbm, tokens),
        (latent_down_hbm, latent_down),
        (rope_down_hbm, rope_down),
        (query_up_hbm, query_up),
        (key_up_hbm, key_up),
        (value_up_hbm, value_up),
        (conv_taps_hbm, conv_taps),
    )
    loads = [pltpu.make_async_copy(a, b, load_sem.at[k]) for k, (a, b) in enumerate(wanted)]
    shards = [pltpu.make_async_copy(a, b, shard_sem.at[k]) for k, (a, b) in enumerate(slots)]
    for copy in loads[:1] + shards + loads[1:]:
        copy.start()

    g_glu = Gather(glu_w, nz, ny, z, y, glu_ps, glu_pr, glu_rs, glu_rr)
    g_ch = Gather(ch_all.at[x], nz, ny, z, y, ch_ps, ch_pr, ch_rs, ch_rr)
    g_keys = Gather(keys_all.at[c], nz, ny, z, y, keys_ps, keys_pr, keys_rs, keys_rr)
    g_out = Gather(out_all, nz, ny, z, y, out_ps, out_pr, out_rs, out_rr)

    def same_places(view):
        return Gather(view, nz, ny, z, y, keys_ps, keys_pr, keys_rs, keys_rr)

    other_keys = same_places(keys_all.at[other])
    sent = []

    def send(src, dst, ssem, rsem, where):
        copy = pltpu.make_async_remote_copy(
            src_ref=src, dst_ref=dst, send_sem=ssem, recv_sem=rsem, device_id=where, device_id_type=MESH
        )
        copy.start()
        sent.append(copy)

    def arrived(dst, ssem, rsem):
        pltpu.make_async_remote_copy(
            src_ref=dst, dst_ref=dst, send_sem=ssem, recv_sem=rsem, device_id=partner, device_id_type=MESH
        ).wait_recv()

    at_row = lax.broadcasted_iota(jnp.int32, (count, ROPE), 0)
    lane = lax.broadcasted_iota(jnp.int32, (count, ROPE), 1)
    place = at_row + sp * count
    grid_row = (place // GRID_W).astype(F32)
    grid_col = lax.rem(place, GRID_W).astype(F32)
    angles = jnp.where(lax.rem(lane, ROPE // 2) < ROPE // 4, grid_row, grid_col) * inv_freq[...]
    wide[0, 0:count, 0:ROPE] = jnp.cos(angles)
    wide[1, 0:count, 0:ROPE] = jnp.sin(angles) * jnp.where(lane < ROPE // 2, -1.0, 1.0)

    loads[0].wait()
    gain = norm_gain[...].astype(F32)[None, :]
    chunk = 32
    for k in range(count // chunk):
        rows = tokens[k * chunk : (k + 1) * chunk, :].astype(F32)
        value = rms(rows, gain).astype(BF16)
        which, first = divmod(k * chunk, half_rows)
        normed4[x, which, first : first + chunk, :] = value

    loads[1].wait()
    loads[2].wait()
    own = normed4[x, c]
    latent = rms(dot(own, latent_down[...]), latent_gain[...].astype(F32)[None, :]).astype(BF16)
    rope_key = dot_t(own, rope_down[...])
    first = pl.multiple_of(c * half_rows, half_rows)
    rope_key = rope_key * wide[0, pl.ds(first, half_rows), 0:ROPE] + swap(rope_key) * wide[
        1, pl.ds(first, half_rows), 0:ROPE
    ]
    quarter = half_rows // 2
    rope_pair = jnp.concatenate([rope_key[:quarter], rope_key[quarter:]], axis=1).astype(BF16)
    for h in (0, 1):
        lo = h * (quarter // 2)
        hi = lo + quarter // 2
        keys_all[c, z, y, h, :, 0:KVR] = latent[lo:hi]
        keys_all[c, z, y, h, :, KVR : 2 * KVR] = latent[quarter + lo : quarter + hi]
        keys_all[c, z, y, h, :, 2 * KVR :] = rope_pair[lo:hi]

    for copy in shards:
        copy.wait()
    edges = has_low.astype(jnp.int32) + has_high.astype(jnp.int32)
    pl.semaphore_wait(barrier, (ny - 1) + (nz - 1) + (NX - 1) + 1 + edges)

    def query_device(a, b):
        return {"sp": jnp.where(first_core, a * ny + b, b * ny + a)}

    def query_copy(phase, d, outgoing):
        if phase == 0:
            b = b_pos if outgoing else lax.rem(b_pos + ny - d, ny)
            ref, where = query_w.at[c, a_pos, b], query_device(a_pos, lax.rem(b_pos + d, ny))
            ssem, rsem = qw_ps.at[d - 1], qw_pr.at[d - 1]
        else:
            a = a_pos if outgoing else lax.rem(a_pos + nz - d, nz)
            ref, where = query_w.at[c, a], query_device(lax.rem(a_pos + d, nz), b_pos)
            ssem, rsem = qw_rs.at[d - 1], qw_rr.at[d - 1]
        return ref, ssem, rsem, where

    def query_start(phase):
        for d in range(1, ny):
            ref, ssem, rsem, where = query_copy(phase, d, True)
            send(ref, ref, ssem, rsem, where)

    query_start(0)
    for way in (0, 1):
        mine = normed4.at[x, c]
        where = {"fs": lax.rem(x + (1 - 2 * way) + NX, NX)}
        send(mine, mine, x_send.at[way], x_recv.at[way], where)
    g_glu.start_first()
    g_ch.start_first()
    g_keys.start_first()
    g_out.start_first()
    for copy in loads[3:]:
        copy.wait()

    def pair_keys(half, way, s):
        block = g_keys.ring_block(half, way, s, False)
        send(block, block, pair_send.at[half, way, s - 1], pair_recv.at[half, way, s - 1], partner)

    def sideways(block, ssem, rsem):
        for w in (0, 1):
            send(block, block, ssem(w), rsem(w), {"fs": lax.rem(x + (1 - 2 * w) + NX, NX)})

    def share(half, way, s):
        block = g_ch.ring_block(half, way, s, False)
        sideways(
            block, lambda w: chx_send.at[w, half, way, s - 1], lambda w: chx_recv.at[w, half, way, s - 1]
        )

    def relay(s):
        plane = same_places(ch_all.at[behind])
        where = {"fs": ahead}
        if s == 0:
            for half in (0, 1):
                block = plane.block(half, y if half else z)
                arrived(block, chx0_send.at[c, half], chx0_recv.at[c, half])
                send(block, block, chr0_send.at[half], chr0_recv.at[half], where)
            return
        for half in (0, 1):
            for way in (0, 1):
                block = plane.ring_block(half, way, s, False)
                arrived(block, chx_send.at[c, half, way, s - 1], chx_recv.at[c, half, way, s - 1])
                send(block, block, chr_send.at[half, way, s - 1], chr_recv.at[half, way, s - 1], where)

    for d in range(1, ny):
        ref, ssem, rsem, where = query_copy(0, d, False)
        arrived(ref, ssem, rsem)
    query_start(1)
    mine = query_w.at[c, a_pos]
    send(mine, mine, qp_send.at[0], qp_recv.at[0], partner)

    last = nz // 2
    g_glu.wait_first()
    g_glu.start_ring(1)
    g_ch.wait_first()
    g_ch.start_ring(1)
    for half in (0, 1):
        sideways(
            g_ch.block(half, y if half else z), lambda w: chx0_send.at[w, half], lambda w: chx0_recv.at[w, half]
        )

    for way in (0, 1):
        src = lax.rem(x - (1 - 2 * way) + NX, NX)
        piece = normed4.at[src, c]
        arrived(piece, x_send.at[way], x_recv.at[way])
        send(piece, piece, xp_send.at[way], xp_recv.at[way], partner)
    onward = normed4.at[behind, c]
    send(onward, onward, x_send.at[2], x_recv.at[2], {"fs": ahead})

    g_keys.wait_first()
    g_keys.start_ring(1)
    for half in (0, 1):
        block = g_keys.block(half, y if half else z)
        send(block, block, pair0_send.at[half], pair0_recv.at[half], partner)

    for d in range(1, nz):
        ref, ssem, rsem, where = query_copy(1, d, False)
        arrived(ref, ssem, rsem)
        send(ref, ref, qp_send.at[d], qp_recv.at[d], partner)

    g_glu.pass_on(1)
    g_ch.pass_on(1, share)
    piece = normed4.at[far, c]
    arrived(piece, x_send.at[2], x_recv.at[2])
    send(piece, piece, xp_send.at[2], xp_recv.at[2], partner)
    g_keys.pass_on(1, pair_keys)

    def to_parts(src, dst, ssem, rsem):
        for d in range(1, NX):
            part = lax.rem(x + d, NX)
            send(src.at[part], dst.at[x], ssem.at[d - 1], rsem.at[d - 1], {"fs": part})

    def from_parts(dst, ssem, rsem):
        for d in range(1, NX):
            arrived(dst.at[lax.rem(x + NX - d, NX)], ssem.at[d - 1], rsem.at[d - 1])

    for d in range(nz):
        theirs = jnp.where(first_core, y, z)
        arrived(query_w.at[other, lax.rem(theirs + nz - d, nz)], qp_send.at[d], qp_recv.at[d])
    for k in range(3):
        src = far if k == 2 else lax.rem(x - (1 - 2 * k) + NX, NX)
        arrived(normed4.at[src, other], xp_send.at[k], xp_recv.at[k])
    pieces = []
    for row in range(nz):
        for column in range(ny):
            pieces += [query_w[0, row, column], query_w[1, column, row]]
    everyone = normed4[...].reshape(NX * count, depth)
    ql_send[...] = dot(everyone, jnp.concatenate(pieces, axis=0)).reshape(NX, count, GROUP)
    to_parts(ql_send, ql_recv, ql_ssem, ql_rsem)
    ql_recv[x] = ql_send[x]

    relay(0)
    g_out.wait_first()
    g_out.start_ring(1)
    g_glu.pass_on(2)
    g_ch.pass_on(2, share)
    g_keys.pass_on(2, pair_keys)
    relay(1)

    from_parts(ql_recv, ql_ssem, ql_rsem)
    latent_query = jnp.concatenate([ql_recv[k] for k in range(NX)], axis=1)
    latent_query = rms(latent_query, query_gain[...].astype(F32)[None, :]).astype(BF16)
    query_all = dot(latent_query, query_up[...])
    cosine = wide[0, 0:count, 0:ROPE]
    sine = wide[1, 0:count, 0:ROPE]
    nothing = jnp.zeros((count, ROPE), F32)
    for h in range(heads):
        start = h * (NOPE + ROPE)
        plain = query_all[:, start : start + NOPE].astype(BF16)
        turned = query_all[:, start + NOPE : start + NOPE + ROPE]
        turned = turned * cosine + swap(turned) * sine
        absorbed = dot_t(plain, key_up[:, h * NOPE : (h + 1) * NOPE]).astype(BF16)
        rows = slice(h * count, (h + 1) * count)
        queries[0, rows, 0:KVR] = absorbed
        queries[1, rows, 0:KVR] = absorbed
        queries[0, rows, KVR:] = jnp.concatenate([turned, nothing], axis=1).astype(BF16)
        queries[1, rows, KVR:] = jnp.concatenate([nothing, turned], axis=1).astype(BF16)

    scale = (NOPE + ROPE) ** (-0.5)
    factor = scale * math.log2(math.e)
    row_max[...] = jnp.full(row_max.shape, -1e30, F32)
    row_sum[...] = jnp.zeros(row_sum.shape, F32)
    acc[...] = jnp.zeros(acc.shape, F32)
    lines = quarter // 2

    def attend(k, carry):
        odd = lax.rem(k, 2)
        step = odd * (lax.div(k, 2) + 1) - (1 - odd) * lax.div(k, 2)
        row = lax.rem(z + step + nz, nz)
        column = lax.rem(y + step + ny, ny)
        pieces, values = [], []
        for core in (0, 1):
            upper = keys_all[core, row, :, 0].reshape(ny * lines, 2 * KVR + 2 * ROPE)
            lower = keys_all[core, :, column, 1].reshape(nz * lines, 2 * KVR + 2 * ROPE)
            block = jnp.concatenate([upper, lower], axis=0)
            tail = block[:, 2 * KVR :]
            for low in (0, 1):
                value = block[:, low * KVR : (low + 1) * KVR]
                pieces.append(dot_t(queries[low], jnp.concatenate([value, tail], axis=1)))
                values.append(value)
        scores = jnp.concatenate(pieces, axis=1)
        before = row_max[...]
        now = jnp.maximum(before, jnp.max(scores, axis=1, keepdims=True))
        shrink = jnp.exp2((before - now) * factor)
        weights = jnp.exp2((scores - jnp.tile(now, (1, scores.shape[1] // 128))) * factor)
        row_sum[...] = row_sum[...] * shrink + jnp.sum(weights, axis=1, keepdims=True)
        row_max[...] = now
        added = dot(weights.astype(BF16), jnp.concatenate(values, axis=0))
        acc[...] = acc[...] * jnp.tile(shrink, (1, KVR // 128)) + added
        return carry

    def pair_arrived(s):
        for half in (0, 1):
            for way in (0, 1):
                ref = other_keys.ring_block(half, way, s, False)
                arrived(ref, pair_send.at[half, way, s - 1], pair_recv.at[half, way, s - 1])

    g_out.pass_on(1)
    for half in (0, 1):
        arrived(other_keys.block(half, y if half else z), pair0_send.at[half], pair0_recv.at[half])
    lax.fori_loop(0, 1, attend, 0)
    g_glu.pass_on(3)
    g_ch.pass_on(3, share)
    g_keys.pass_on(3, pair_keys)
    relay(2)
    g_out.pass_on(2)
    pair_arrived(1)
    lax.fori_loop(1, 3, attend, 0)

    g_glu.pass_on(4)
    g_ch.pass_on(4, share)
    g_keys.pass_on(4, pair_keys)
    relay(3)
    glu_weights = glu_w[...].reshape(depth, 2 * GROUP)
    for j in range(NX):
        product = dot(normed4[j].reshape(count, depth), glu_weights)
        gated[j, HALO : HALO + count, :] = (product[:, :GROUP] * jax.nn.sigmoid(product[:, GROUP:])).astype(BF16)

    low_src, high_src = gated.at[:, pl.ds(HALO, HALO)], gated.at[:, pl.ds(count, HALO)]
    low_dst, high_dst = gated.at[:, pl.ds(0, HALO)], gated.at[:, pl.ds(HALO + count, HALO)]

    def halo_copy(up):
        src, dst = (high_src, low_dst) if up else (low_src, high_dst)
        k = 0 if up else 1
        return pltpu.make_async_remote_copy(
            src_ref=src,
            dst_ref=dst,
            send_sem=halo_ssem.at[k],
            recv_sem=halo_rsem.at[k],
            device_id={"sp": sp + 1 if up else sp - 1},
            device_id_type=MESH,
        )

    @pl.when(has_high)
    def _():
        halo_copy(True).start()

    @pl.when(has_low)
    def _():
        halo_copy(False).start()

    edge = jnp.zeros((NX, HALO, GROUP), BF16)

    @pl.when(jnp.logical_not(has_low))
    def _():
        gated[:, 0:HALO, :] = edge

    @pl.when(jnp.logical_not(has_high))
    def _():
        gated[:, HALO + count :, :] = edge

    pair_arrived(2)
    lax.fori_loop(3, 5, attend, 0)
    g_out.pass_on(3)
    relay(4)

    @pl.when(has_low)
    def _():
        halo_copy(True).wait_recv()

    @pl.when(has_high)
    def _():
        halo_copy(False).wait_recv()

    reach = conv_taps.shape[0] // 2
    taps = conv_taps[:, columns].astype(F32)
    gains = group_gain[...].astype(F32)[None, :]
    channel_gain = gains[:, :GROUP]
    for k in range(1, NX):
        channel_gain = jnp.where(x == k, gains[:, k * GROUP : (k + 1) * GROUP], channel_gain)
    for j in range(NX):
        wide[j, :, :] = gated[j].astype(F32)
        total = jnp.zeros((count, GROUP), F32)
        for t in range(2 * reach + 1):
            lo = HALO - reach + t
            total = total + wide[j, lo : lo + count, :] * taps[t : t + 1, :]
        centred = total - jnp.mean(total, axis=-1, keepdims=True)
        spread = jnp.mean(centred * centred, axis=-1, keepdims=True)
        conv_send[j] = jax.nn.silu(centred * lax.rsqrt(spread + EPS) * channel_gain).astype(BF16)
    to_parts(conv_send, conv_recv, cv_ssem, cv_rsem)
    conv_recv[x] = conv_send[x]

    pair_arrived(3)
    lax.fori_loop(5, 7, attend, 0)
    pair_arrived(4)
    lax.fori_loop(7, 8, attend, 0)

    for h in range(heads):
        rows = slice(h * count, (h + 1) * count)
        attended = (acc[rows, :] / jnp.tile(row_sum[rows, :], (1, KVR // 128))).astype(BF16)
        head_out[:, h * VDIM : (h + 1) * VDIM] = dot(attended, value_up[:, h * VDIM : (h + 1) * VDIM]).astype(BF16)
        logs = row_max[rows, :] * scale + jnp.log(row_sum[rows, :])
        log_weight[h : h + 1, :] = jnp.transpose(logs)[0:1, :]

    from_parts(conv_recv, cv_ssem, cv_rsem)
    mixed = jnp.concatenate([head_out[...]] + [conv_recv[k] for k in range(NX)], axis=1)
    zs = nz // 2
    width = zs * ny * 2 * out_all.shape[3]
    g_out.pass_on(4)
    for plane, sems in ((ahead, (chx_send, chx_recv, chx0_send, chx0_recv)), (far, None)):
        places = same_places(ch_all.at[plane])
        for half in (0, 1):
            block = places.block(half, y if half else z)
            if sems is None:
                arrived(block, chr0_send.at[half], chr0_recv.at[half])
            else:
                arrived(block, chx0_send.at[other, half], chx0_recv.at[other, half])
            for s in range(1, last + 1):
                for way in (0, 1):
                    block = places.ring_block(half, way, s, False)
                    if sems is None:
                        arrived(block, chr_send.at[half, way, s - 1], chr_recv.at[half, way, s - 1])
                    else:
                        arrived(
                            block, chx_send.at[other, half, way, s - 1], chx_recv.at[other, half, way, s - 1]
                        )

    def columns_of(core):
        rows = pl.ds(core * zs, zs)
        parts = [out_all[rows].reshape(width, heads * VDIM)]
        parts += [ch_all[k, rows].reshape(width, GROUP) for k in range(NX)]
        return dot_t(mixed, jnp.concatenate(parts, axis=1)).astype(BF16)

    part_send[...] = columns_of(other)
    send(part_send, part_recv, fin_sem.at[0], fin_sem.at[1], partner)
    kept[...] = columns_of(c)
    arrived(part_recv, fin_sem.at[0], fin_sem.at[1])

    for copy in sent:
        copy.wait_send()
    for gather in (g_glu, g_ch, g_keys, g_out):
        gather.finish()

    @pl.when(has_high)
    def _():
        halo_copy(True).wait_send()

    @pl.when(has_low)
    def _():
        halo_copy(False).wait_send()


def per_device(
    nz,
    ny,
    tokens,
    norm_gain,
    query_down,
    query_gain,
    latent_down,
    latent_gain,
    rope_down,
    query_up,
    key_up,
    value_up,
    glu_value,
    glu_gate,
    conv_taps,
    group_gain,
    head_proj,
    channel_proj,
):
    count, depth = tokens.shape
    heads = key_up.shape[1] // NOPE

    def halves(a):
        return a.reshape(2, a.shape[0] // 2, a.shape[1])

    freq = (BASE ** (-np.arange(ROPE // 4, dtype=np.float64) / (ROPE // 4))).astype(np.float32)
    whole = (tokens, latent_down, rope_down.T, query_up, key_up, value_up, conv_taps)
    shards = [halves(a) for a in (query_down, glu_value, glu_gate, head_proj.T, channel_proj.T)]
    gains = (norm_gain, query_gain, latent_gain, group_gain, jnp.asarray(np.tile(freq, 4)[None, :]))
    shard = query_down.shape[0] // 2
    out_cols = head_proj.shape[1]
    half_cols = nz * ny * out_cols // 2
    last = nz // 2
    dma = pltpu.SemaphoreType.DMA
    vmem = pl.BlockSpec(memory_space=pltpu.VMEM)
    hbm = pl.BlockSpec(memory_space=pltpu.HBM)

    def buf(*shape, dtype=BF16):
        return pltpu.VMEM(shape, dtype)

    ring = [dma((2, ny - 1)), dma((2, ny - 1)), dma((2, 2, last)), dma((2, 2, last))]
    scratch = [
        buf(NX, 2, count // 2, depth),
        buf(2, nz, ny, shard, GROUP),
        buf(nz, ny, 2, shard, 2 * GROUP),
        buf(NX, nz, ny, 2, out_cols // 2, GROUP),
        buf(2, nz, ny, 2, count // 8, 2 * KVR + 2 * ROPE),
        buf(nz, ny, 2, out_cols // 2, heads * VDIM),
        buf(NX, count, GROUP, dtype=F32),
        buf(NX, count, GROUP, dtype=F32),
        buf(NX, count + 2 * HALO, GROUP),
        buf(NX, count + 2 * HALO, GROUP, dtype=F32),
        buf(NX, count, GROUP),
        buf(NX, count, GROUP),
        buf(2, heads * count, KVR + 2 * ROPE),
        buf(heads * count, 128, dtype=F32),
        buf(heads * count, 128, dtype=F32),
        buf(heads * count, KVR, dtype=F32),
        buf(count, heads * VDIM),
        buf(count, half_cols),
        *[buf(*a.shape) for a in whole],
        dma((len(whole),)),
        dma((5,)),
        *[dma((ny - 1,))] * 4,
        *ring * 4,
        *[dma((nz,))] * 2,
        *[dma((2, 2, 2, last))] * 2,
        *[dma((2, 2))] * 2,
        *[dma((2, 2, last))] * 2,
        *[dma((2,))] * 2,
        *[dma((2, 2, last))] * 2,
        *[dma((2,))] * 2,
        *[dma((3,))] * 8,
        *[dma((2,))] * 3,
    ]
    kept, came, log_weight = pl.pallas_call(
        functools.partial(kernel, nz, ny),
        out_shape=(
            jax.ShapeDtypeStruct((count, half_cols), BF16),
            jax.ShapeDtypeStruct((count, half_cols), BF16),
            jax.ShapeDtypeStruct((heads, count), F32),
        ),
        in_specs=[hbm] * (len(whole) + len(shards)) + [vmem] * len(gains),
        out_specs=(vmem, vmem, vmem),
        scratch_shapes=scratch,
        compiler_params=pltpu.CompilerParams(
            collective_id=0, has_side_effects=True, vmem_limit_bytes=60 * 1024 * 1024
        ),
    )(*whole, *shards, *gains)
    return (kept.astype(F32) + came.astype(F32)).astype(BF16), log_weight


def solution(mesh):
    sp = mesh.shape["sp"]
    ny = math.isqrt(sp)
    nz = sp // ny
    in_specs = (
        P(("fs", "sp"), None),
        P(),
        P("sp", None),
        P(),
        P(),
        P(),
        P(),
        P(None, "tp"),
        P(None, "tp"),
        P(None, "tp"),
        P("sp", "tp"),
        P("sp", "tp"),
        P(None, "tp"),
        P("tp"),
        P("tp", "sp"),
        P("tp", "sp"),
    )
    out_specs = (P(("fs", "sp"), "tp"), P("tp", ("fs", "sp")))
    return jax.shard_map(
        functools.partial(per_device, nz, ny), mesh=mesh, in_specs=in_specs, out_specs=out_specs, check_vma=False
    )
```

```python
import functools
import math

import jax
import jax.numpy as jnp
import numpy as np
from jax import lax
from jax.experimental import pallas as pl
from jax.experimental.pallas import tpu as pltpu
from jax.sharding import PartitionSpec as P

NOPE = 128
ROPE = 64
VDIM = 128
KVR = 256
GROUP = 128
GRID_W = 64
EPS = 1e-06
BASE = 10000.0
HALO = 16
NX = 4
F32 = jnp.float32
BF16 = jnp.bfloat16
MESH = pl.DeviceIdType.MESH


def dot(a, b):
    return jnp.dot(a, b, preferred_element_type=F32)


def dot_t(a, b):
    return lax.dot_general(a, b, (((1,), (1,)), ((), ())), preferred_element_type=F32)


def rms(values, gain):
    inv = lax.rsqrt(jnp.mean(values * values, axis=-1, keepdims=True) + EPS)
    return values * inv * gain


def swap(v):
    half = v.shape[-1] // 2
    return jnp.concatenate([v[:, half:], v[:, :half]], axis=-1)


def await_bytes(ref, sem):
    pltpu.make_async_remote_copy(
        src_ref=ref,
        dst_ref=ref,
        send_sem=sem,
        recv_sem=sem,
        device_id={"tp": 1 - lax.axis_index("tp")},
        device_id_type=MESH,
    ).wait_recv()


class Gather:
    def __init__(self, view, nz, ny, z, y, sems, steps):
        self.view, self.size, self.pos = view, (nz, ny), (z, y)
        self.sems, self.steps = sems, steps

    def device(self, axis, k):
        z, y = (k, self.pos[1]) if axis == 0 else (self.pos[0], k)
        return {"sp": z * self.size[1] + y}

    def send(self, ref, k, arrival, where):
        pltpu.make_async_remote_copy(
            src_ref=ref,
            dst_ref=ref,
            send_sem=self.sems.at[k],
            recv_sem=arrival,
            device_id=where,
            device_id_type=MESH,
        ).start()

    def start_first(self):
        z, y = self.pos
        for half in (0, 1):
            axis = 1 - half
            n = self.size[axis]
            for d in range(1, n):
                where = self.device(axis, lax.rem(self.pos[axis] + d, n))
                self.send(self.view.at[z, y, half], 0, self.sems.at[1], where)

    def wait_first(self):
        await_bytes(self.view.at[0, pl.ds(0, self.size[1] - 1)], self.sems.at[1])

    def block(self, half, k, part=None):
        n = self.size[1 - half]
        rows = slice(None) if part is None else pl.ds(part * (n // 2), n // 2)
        return self.view.at[k, rows, 0] if half == 0 else self.view.at[rows, k, 1]

    def ring_block(self, half, way, s, outgoing=False):
        n = self.size[half]
        back = s - 1 if outgoing else s
        k = lax.rem(self.pos[half] - (1 - 2 * way) * back + n, n)
        return self.block(half, k, way if s == n // 2 else None)

    def blocks(self, s):
        if s == 0:
            return [self.block(0, self.pos[0]), self.block(1, self.pos[1])]
        return [self.ring_block(half, way, s) for half in (0, 1) for way in (0, 1)]

    def like(self, s):
        return self.view.at[0] if s in (0, self.size[0] // 2) else self.view.at[pl.ds(0, 2)]

    def start_ring(self, s):
        for half in (0, 1):
            n = self.size[half]
            for way in (0, 1):
                where = self.device(half, lax.rem(self.pos[half] + (1 - 2 * way) + n, n))
                self.send(self.ring_block(half, way, s, True), 2, self.steps.at[s], where)

    def pass_on(self, s, each=None):
        await_bytes(self.like(s), self.steps.at[s])
        if s < self.size[0] // 2:
            self.start_ring(s + 1)
        if each is not None:
            each(s)

    def finish(self):
        n = self.size[0]
        await_bytes(self.view.at[0, pl.ds(0, n - 1)], self.sems.at[0])
        await_bytes(self.view.at[pl.ds(0, n - 1)], self.sems.at[2])


def kernel(
    nz,
    ny,
    tokens_hbm,
    latent_down_hbm,
    rope_down_hbm,
    query_up_hbm,
    key_up_hbm,
    value_up_hbm,
    conv_taps_hbm,
    query_down,
    glu_value,
    glu_gate,
    head_proj,
    channel_proj,
    norm_gain_hbm,
    query_gain_hbm,
    latent_gain_hbm,
    group_gain_hbm,
    inv_freq_hbm,
    kept,
    part_recv,
    log_weight,
    normed4,
    query_w,
    glu_w,
    ch_all,
    keys_all,
    out_all,
    ql_send,
    ql_recv,
    gated,
    wide,
    conv_send,
    conv_recv,
    queries,
    row_max,
    row_sum,
    acc,
    head_out,
    part_send,
    tokens,
    latent_down,
    rope_down,
    query_up,
    key_up,
    value_up,
    conv_taps,
    norm_gain,
    query_gain,
    latent_gain,
    group_gain,
    inv_freq,
    load_sem,
    shard_sem,
    query_sem,
    glu_sems,
    glu_steps,
    ch_sems,
    ch_steps,
    keys_sems,
    keys_steps,
    out_sems,
    out_steps,
    side_send,
    side_recv,
    relay_send,
    relay_recv,
    pair_send,
    pair_recv,
    x_send,
    x_recv,
    xp_send,
    xp_recv,
    ql_sem,
    cv_sem,
    halo_ssem,
    halo_rsem,
    fin_sem,
):
    sp = lax.axis_index("sp")
    x = lax.axis_index("fs")
    c = lax.axis_index("tp")
    z, y = sp // ny, lax.rem(sp, ny)
    other = 1 - c
    count, depth = tokens.shape
    half_rows = count // 2
    heads = key_up.shape[1] // NOPE
    partner = {"tp": other}
    turn = 1 - 2 * c
    behind, ahead, far = lax.rem(x - turn + NX, NX), lax.rem(x + turn + NX, NX), lax.rem(x + 2, NX)

    barrier = pltpu.get_barrier_semaphore()

    def greet(**where):
        pl.semaphore_signal(barrier, inc=1, device_id=where, device_id_type=MESH)

    for d in range(1, ny):
        greet(sp=z * ny + lax.rem(y + d, ny))
    for d in range(1, nz):
        greet(sp=lax.rem(z + d, nz) * ny + y)
    for d in range(1, NX):
        greet(fs=lax.rem(x + d, NX))
    greet(tp=other)
    has_low = sp > 0
    has_high = sp < nz * ny - 1

    @pl.when(has_low)
    def _():
        greet(sp=sp - 1)

    @pl.when(has_high)
    def _():
        greet(sp=sp + 1)

    first_core = c == 0
    a_pos, b_pos = jnp.where(first_core, z, y), jnp.where(first_core, y, z)
    columns = pl.ds(pl.multiple_of(x * GROUP, GROUP), GROUP)
    slots = (
        (query_down.at[c, :, columns], query_w.at[c, a_pos, b_pos]),
        (glu_value.at[:, :, columns], glu_w.at[z, y, :, :, pl.ds(0, GROUP)]),
        (glu_gate.at[:, :, columns], glu_w.at[z, y, :, :, pl.ds(GROUP, GROUP)]),
        (channel_proj.at[:, :, columns], ch_all.at[x, z, y]),
        (head_proj, out_all.at[z, y]),
    )
    wanted = (
        (tokens_hbm, tokens),
        (latent_down_hbm, latent_down),
        (rope_down_hbm, rope_down),
        (query_up_hbm, query_up),
        (key_up_hbm, key_up),
        (value_up_hbm, value_up),
        (conv_taps_hbm, conv_taps),
        (norm_gain_hbm, norm_gain),
        (query_gain_hbm, query_gain),
        (latent_gain_hbm, latent_gain),
        (group_gain_hbm, group_gain),
        (inv_freq_hbm, inv_freq),
    )
    loads = [pltpu.make_async_copy(a, b, load_sem.at[k]) for k, (a, b) in enumerate(wanted)]
    shards = [pltpu.make_async_copy(a, b, shard_sem.at[k]) for k, (a, b) in enumerate(slots)]
    for copy in shards + loads:
        copy.start()

    g_glu = Gather(glu_w, nz, ny, z, y, glu_sems, glu_steps)
    g_ch = Gather(ch_all.at[x], nz, ny, z, y, ch_sems, ch_steps)
    g_keys = Gather(keys_all.at[c], nz, ny, z, y, keys_sems, keys_steps)
    g_out = Gather(out_all, nz, ny, z, y, out_sems, out_steps)
    sent = []

    def send(src, dst, ssem, rsem, where):
        copy = pltpu.make_async_remote_copy(
            src_ref=src, dst_ref=dst, send_sem=ssem, recv_sem=rsem, device_id=where, device_id_type=MESH
        )
        copy.start()
        return copy

    def arrived(dst, ssem, rsem):
        pltpu.make_async_remote_copy(
            src_ref=dst, dst_ref=dst, send_sem=ssem, recv_sem=rsem, device_id=partner, device_id_type=MESH
        ).wait_recv()

    for copy in shards:
        copy.wait()
    edges = has_low.astype(jnp.int32) + has_high.astype(jnp.int32)
    pl.semaphore_wait(barrier, (ny - 1) + (nz - 1) + (NX - 1) + 1 + edges)

    def query_start(phase):
        for d in range(1, ny):
            if phase == 0:
                a, b = a_pos, lax.rem(b_pos + d, ny)
                ref = query_w.at[c, a_pos, b_pos]
            else:
                a, b = lax.rem(a_pos + d, nz), b_pos
                ref = query_w.at[c, a_pos]
            where = {"sp": jnp.where(first_core, a * ny + b, b * ny + a)}
            send(ref, ref, query_sem.at[2 * phase], query_sem.at[2 * phase + 1], where)

    query_start(0)
    g_glu.start_first()
    g_ch.start_first()
    loads[0].wait()
    loads[7].wait()
    gain = norm_gain[...].astype(F32)[None, :]
    chunk = 32
    for k in range(count // chunk):
        rows = tokens[k * chunk : (k + 1) * chunk, :].astype(F32)
        value = rms(rows, gain).astype(BF16)
        which, first = divmod(k * chunk, half_rows)
        normed4[x, which, first : first + chunk, :] = value

    for way in (0, 1):
        mine = normed4.at[x, c]
        where = {"fs": lax.rem(x + (1 - 2 * way) + NX, NX)}
        sent.append(send(mine, mine, x_send.at[way], x_recv.at[way], where))
    at_row = lax.broadcasted_iota(jnp.int32, (count, ROPE), 0)
    lane = lax.broadcasted_iota(jnp.int32, (count, ROPE), 1)
    place = at_row + sp * count
    grid_row = (place // GRID_W).astype(F32)
    grid_col = lax.rem(place, GRID_W).astype(F32)
    loads[11].wait()
    angles = jnp.where(lax.rem(lane, ROPE // 2) < ROPE // 4, grid_row, grid_col) * inv_freq[...]
    wide[0, 0:count, 0:ROPE] = jnp.cos(angles)
    wide[1, 0:count, 0:ROPE] = jnp.sin(angles) * jnp.where(lane < ROPE // 2, -1.0, 1.0)

    loads[1].wait()
    loads[2].wait()
    loads[9].wait()
    own = normed4[x, c]
    latent = rms(dot(own, latent_down[...]), latent_gain[...].astype(F32)[None, :]).astype(BF16)
    rope_key = dot_t(own, rope_down[...])
    first = pl.multiple_of(c * half_rows, half_rows)
    rope_key = rope_key * wide[0, pl.ds(first, half_rows), 0:ROPE] + swap(rope_key) * wide[
        1, pl.ds(first, half_rows), 0:ROPE
    ]
    quarter = half_rows // 2
    rope_pair = jnp.concatenate([rope_key[:quarter], rope_key[quarter:]], axis=1).astype(BF16)
    for h in (0, 1):
        lo = h * (quarter // 2)
        hi = lo + quarter // 2
        keys_all[c, z, y, h, :, 0:KVR] = latent[lo:hi]
        keys_all[c, z, y, h, :, KVR : 2 * KVR] = latent[quarter + lo : quarter + hi]
        keys_all[c, z, y, h, :, 2 * KVR :] = rope_pair[lo:hi]

    g_keys.start_first()
    g_out.start_first()
    for copy in loads[3:7] + [loads[8], loads[10]]:
        copy.wait()

    def pair_keys(s):
        for block in g_keys.blocks(s):
            send(block, block, pair_send.at[0], pair_recv.at[s], partner)

    def pair_arrived(s):
        await_bytes(g_keys.like(s), pair_recv.at[s])

    def share(s):
        for block in g_ch.blocks(s):
            for w in (0, 1):
                where = {"fs": lax.rem(x + (1 - 2 * w) + NX, NX)}
                send(block, block, side_send.at[0], side_recv.at[w, s], where)

    passing = Gather(ch_all.at[behind], nz, ny, z, y, ch_sems, ch_steps)

    def relay(s):
        await_bytes(g_ch.like(s), side_recv.at[c, s])
        for block in passing.blocks(s):
            send(block, block, relay_send.at[0], relay_recv.at[s], {"fs": ahead})

    await_bytes(query_w.at[0, 0, pl.ds(0, ny - 1)], query_sem.at[1])
    query_start(1)

    last = nz // 2
    g_glu.wait_first()
    g_glu.start_ring(1)
    g_ch.wait_first()
    g_ch.start_ring(1)

    for way in (0, 1):
        src = lax.rem(x - (1 - 2 * way) + NX, NX)
        piece = normed4.at[src, c]
        arrived(piece, x_send.at[way], x_recv.at[way])
        sent.append(send(piece, piece, xp_send.at[way], xp_recv.at[way], partner))
    onward = normed4.at[behind, c]
    sent.append(send(onward, onward, x_send.at[2], x_recv.at[2], {"fs": ahead}))

    g_keys.wait_first()
    g_keys.start_ring(1)
    pair_keys(0)

    g_out.wait_first()
    g_out.start_ring(1)

    await_bytes(query_w.at[0, pl.ds(0, nz - 1)], query_sem.at[3])
    sent.append(send(query_w.at[c], query_w.at[c], query_sem.at[4], query_sem.at[5], partner))
    piece = normed4.at[far, c]
    arrived(piece, x_send.at[2], x_recv.at[2])
    sent.append(send(piece, piece, xp_send.at[2], xp_recv.at[2], partner))
    g_glu.pass_on(1)
    g_ch.pass_on(1)

    def to_parts(src, dst, sems):
        for d in range(1, NX):
            part = lax.rem(x + d, NX)
            send(src.at[part], dst.at[x], sems.at[0], sems.at[1], {"fs": part})

    def from_parts(dst, sems):
        await_bytes(dst.at[pl.ds(0, NX - 1)], sems.at[1])

    await_bytes(query_w.at[other], query_sem.at[5])
    for k in range(3):
        src = far if k == 2 else lax.rem(x - (1 - 2 * k) + NX, NX)
        arrived(normed4.at[src, other], xp_send.at[k], xp_recv.at[k])
    pieces = []
    for row in range(nz):
        for column in range(ny):
            pieces += [query_w[0, row, column], query_w[1, column, row]]
    everyone = normed4[...].reshape(NX * count, depth)
    ql_send[...] = dot(everyone, jnp.concatenate(pieces, axis=0)).reshape(NX, count, GROUP)
    to_parts(ql_send, ql_recv, ql_sem)
    ql_recv[x] = ql_send[x]
    share(0)
    share(1)

    g_keys.pass_on(1, pair_keys)

    from_parts(ql_recv, ql_sem)
    latent_query = jnp.concatenate([ql_recv[k] for k in range(NX)], axis=1)
    latent_query = rms(latent_query, query_gain[...].astype(F32)[None, :]).astype(BF16)
    query_all = dot(latent_query, query_up[...])
    cosine = wide[0, 0:count, 0:ROPE]
    sine = wide[1, 0:count, 0:ROPE]
    nothing = jnp.zeros((count, ROPE), F32)
    for h in range(heads):
        start = h * (NOPE + ROPE)
        plain = query_all[:, start : start + NOPE].astype(BF16)
        turned = query_all[:, start + NOPE : start + NOPE + ROPE]
        turned = turned * cosine + swap(turned) * sine
        absorbed = dot_t(plain, key_up[:, h * NOPE : (h + 1) * NOPE]).astype(BF16)
        rows = slice(h * count, (h + 1) * count)
        queries[0, rows, 0:KVR] = absorbed
        queries[1, rows, 0:KVR] = absorbed
        queries[0, rows, KVR:] = jnp.concatenate([turned, nothing], axis=1).astype(BF16)
        queries[1, rows, KVR:] = jnp.concatenate([nothing, turned], axis=1).astype(BF16)

    scale = (NOPE + ROPE) ** (-0.5)
    factor = scale * math.log2(math.e)
    row_max[...] = jnp.full(row_max.shape, -1e30, F32)
    row_sum[...] = jnp.zeros(row_sum.shape, F32)
    acc[...] = jnp.zeros(acc.shape, F32)
    lines = quarter // 2

    def attend(k, carry):
        odd = lax.rem(k, 2)
        step = odd * (lax.div(k, 2) + 1) - (1 - odd) * lax.div(k, 2)
        row = lax.rem(z + step + nz, nz)
        column = lax.rem(y + step + ny, ny)
        pieces, values = [], []
        for core in (0, 1):
            upper = keys_all[core, row, :, 0].reshape(ny * lines, 2 * KVR + 2 * ROPE)
            lower = keys_all[core, :, column, 1].reshape(nz * lines, 2 * KVR + 2 * ROPE)
            block = jnp.concatenate([upper, lower], axis=0)
            tail = block[:, 2 * KVR :]
            for low in (0, 1):
                value = block[:, low * KVR : (low + 1) * KVR]
                pieces.append(dot_t(queries[low], jnp.concatenate([value, tail], axis=1)))
                values.append(value)
        scores = jnp.concatenate(pieces, axis=1)
        before = row_max[...]
        now = jnp.maximum(before, jnp.max(scores, axis=1, keepdims=True))
        shrink = jnp.exp2((before - now) * factor)
        weights = jnp.exp2((scores - jnp.tile(now, (1, scores.shape[1] // 128))) * factor)
        row_sum[...] = row_sum[...] * shrink + jnp.sum(weights, axis=1, keepdims=True)
        row_max[...] = now
        added = dot(weights.astype(BF16), jnp.concatenate(values, axis=0))
        acc[...] = acc[...] * jnp.tile(shrink, (1, KVR // 128)) + added
        return carry

    g_glu.pass_on(2)
    g_ch.pass_on(2, share)
    g_out.pass_on(1)
    pair_arrived(0)
    lax.fori_loop(0, 1, attend, 0)
    pair_arrived(1)
    g_keys.pass_on(2, pair_keys)
    lax.fori_loop(1, 2, attend, 0)
    g_glu.pass_on(3)
    g_ch.pass_on(3, share)
    relay(0)
    relay(1)
    lax.fori_loop(2, 3, attend, 0)
    g_out.pass_on(2)
    pair_arrived(2)
    lax.fori_loop(3, 4, attend, 0)

    g_glu.pass_on(4)
    g_ch.pass_on(4, share)
    relay(2)
    glu_weights = glu_w[...].reshape(depth, 2 * GROUP)
    for j in range(NX):
        product = dot(normed4[j].reshape(count, depth), glu_weights)
        gated[j, HALO : HALO + count, :] = (product[:, :GROUP] * jax.nn.sigmoid(product[:, GROUP:])).astype(BF16)

    low_src, high_src = gated.at[:, pl.ds(HALO, HALO)], gated.at[:, pl.ds(count, HALO)]
    low_dst, high_dst = gated.at[:, pl.ds(0, HALO)], gated.at[:, pl.ds(HALO + count, HALO)]

    def halo_copy(up):
        src, dst = (high_src, low_dst) if up else (low_src, high_dst)
        k = 0 if up else 1
        return pltpu.make_async_remote_copy(
            src_ref=src,
            dst_ref=dst,
            send_sem=halo_ssem.at[k],
            recv_sem=halo_rsem.at[k],
            device_id={"sp": sp + 1 if up else sp - 1},
            device_id_type=MESH,
        )

    @pl.when(has_high)
    def _():
        halo_copy(True).start()

    @pl.when(has_low)
    def _():
        halo_copy(False).start()

    edge = jnp.zeros((NX, HALO, GROUP), BF16)

    @pl.when(jnp.logical_not(has_low))
    def _():
        gated[:, 0:HALO, :] = edge

    @pl.when(jnp.logical_not(has_high))
    def _():
        gated[:, HALO + count :, :] = edge

    g_keys.pass_on(3, pair_keys)
    lax.fori_loop(4, 5, attend, 0)
    relay(3)
    g_out.pass_on(3)

    @pl.when(has_low)
    def _():
        halo_copy(True).wait_recv()

    @pl.when(has_high)
    def _():
        halo_copy(False).wait_recv()

    reach = conv_taps.shape[0] // 2
    taps = conv_taps[:, columns].astype(F32)
    gains = group_gain[...].astype(F32)[None, :]
    channel_gain = gains[:, :GROUP]
    for k in range(1, NX):
        channel_gain = jnp.where(x == k, gains[:, k * GROUP : (k + 1) * GROUP], channel_gain)
    for j in range(NX):
        wide[j, :, :] = gated[j].astype(F32)
        total = jnp.zeros((count, GROUP), F32)
        for t in range(2 * reach + 1):
            lo = HALO - reach + t
            total = total + wide[j, lo : lo + count, :] * taps[t : t + 1, :]
        centred = total - jnp.mean(total, axis=-1, keepdims=True)
        spread = jnp.mean(centred * centred, axis=-1, keepdims=True)
        conv_send[j] = jax.nn.silu(centred * lax.rsqrt(spread + EPS) * channel_gain).astype(BF16)
    to_parts(conv_send, conv_recv, cv_sem)
    conv_recv[x] = conv_send[x]

    pair_arrived(3)
    lax.fori_loop(5, 6, attend, 0)
    g_keys.pass_on(4, pair_keys)
    relay(4)
    lax.fori_loop(6, 7, attend, 0)
    pair_arrived(4)
    lax.fori_loop(7, 8, attend, 0)

    for h in range(heads):
        rows = slice(h * count, (h + 1) * count)
        attended = (acc[rows, :] / jnp.tile(row_sum[rows, :], (1, KVR // 128))).astype(BF16)
        head_out[:, h * VDIM : (h + 1) * VDIM] = dot(attended, value_up[:, h * VDIM : (h + 1) * VDIM]).astype(BF16)
        logs = row_max[rows, :] * scale + jnp.log(row_sum[rows, :])
        log_weight[h : h + 1, :] = jnp.transpose(logs)[0:1, :]

    from_parts(conv_recv, cv_sem)
    mixed = jnp.concatenate([head_out[...]] + [conv_recv[k] for k in range(NX)], axis=1)
    zs = nz // 2
    width = zs * ny * 2 * out_all.shape[3]
    g_out.pass_on(4)
    for s in range(last + 1):
        await_bytes(g_ch.like(s), side_recv.at[other, s])
        await_bytes(g_ch.like(s), relay_recv.at[s])

    def columns_of(core):
        rows = pl.ds(core * zs, zs)
        parts = [out_all[rows].reshape(width, heads * VDIM)]
        parts += [ch_all[k, rows].reshape(width, GROUP) for k in range(NX)]
        return dot_t(mixed, jnp.concatenate(parts, axis=1)).astype(BF16)

    part_send[...] = columns_of(other)
    sent.append(send(part_send, part_recv, fin_sem.at[0], fin_sem.at[1], partner))
    kept[...] = columns_of(c)
    arrived(part_recv, fin_sem.at[0], fin_sem.at[1])

    for copy in sent:
        copy.wait_send()
    await_bytes(query_w.at[0, 0, pl.ds(0, ny - 1)], query_sem.at[0])
    await_bytes(query_w.at[0, pl.ds(0, nz - 1)], query_sem.at[2])
    await_bytes(keys_all.at[0], pair_send.at[0])
    await_bytes(ch_all.at[pl.ds(0, 2)], side_send.at[0])
    await_bytes(ch_all.at[0], relay_send.at[0])
    await_bytes(ql_send.at[pl.ds(0, NX - 1)], ql_sem.at[0])
    await_bytes(conv_send.at[pl.ds(0, NX - 1)], cv_sem.at[0])
    g_glu.finish()
    g_ch.finish()
    g_keys.finish()
    g_out.finish()

    @pl.when(has_high)
    def _():
        halo_copy(True).wait_send()

    @pl.when(has_low)
    def _():
        halo_copy(False).wait_send()


def per_device(
    nz,
    ny,
    tokens,
    norm_gain,
    query_down,
    query_gain,
    latent_down,
    latent_gain,
    rope_down,
    query_up,
    key_up,
    value_up,
    glu_value,
    glu_gate,
    conv_taps,
    group_gain,
    head_proj,
    channel_proj,
):
    count, depth = tokens.shape
    heads = key_up.shape[1] // NOPE

    def halves(a):
        return a.reshape(2, a.shape[0] // 2, a.shape[1])

    freq = (BASE ** (-np.arange(ROPE // 4, dtype=np.float64) / (ROPE // 4))).astype(np.float32)
    whole = (tokens, latent_down, rope_down.T, query_up, key_up, value_up, conv_taps)
    shards = [halves(a) for a in (query_down, glu_value, glu_gate, head_proj.T, channel_proj.T)]
    gains = (norm_gain, query_gain, latent_gain, group_gain, jnp.asarray(np.tile(freq, 4)[None, :]))
    shard = query_down.shape[0] // 2
    out_cols = head_proj.shape[1]
    half_cols = nz * ny * out_cols // 2
    last = nz // 2
    dma = pltpu.SemaphoreType.DMA
    vmem = pl.BlockSpec(memory_space=pltpu.VMEM)
    hbm = pl.BlockSpec(memory_space=pltpu.HBM)

    def buf(*shape, dtype=BF16):
        return pltpu.VMEM(shape, dtype)

    scratch = [
        buf(NX, 2, count // 2, depth),
        buf(2, nz, ny, shard, GROUP),
        buf(nz, ny, 2, shard, 2 * GROUP),
        buf(NX, nz, ny, 2, out_cols // 2, GROUP),
        buf(2, nz, ny, 2, count // 8, 2 * KVR + 2 * ROPE),
        buf(nz, ny, 2, out_cols // 2, heads * VDIM),
        buf(NX, count, GROUP, dtype=F32),
        buf(NX, count, GROUP, dtype=F32),
        buf(NX, count + 2 * HALO, GROUP),
        buf(NX, count + 2 * HALO, GROUP, dtype=F32),
        buf(NX, count, GROUP),
        buf(NX, count, GROUP),
        buf(2, heads * count, KVR + 2 * ROPE),
        buf(heads * count, 128, dtype=F32),
        buf(heads * count, 128, dtype=F32),
        buf(heads * count, KVR, dtype=F32),
        buf(count, heads * VDIM),
        buf(count, half_cols),
        *[buf(*a.shape, dtype=a.dtype) for a in whole + gains],
        dma((len(whole + gains),)),
        dma((5,)),
        dma((6,)),
        *[dma((3,)), dma((last + 1,))] * 4,
        dma((1,)),
        dma((2, last + 1)),
        dma((1,)),
        dma((last + 1,)),
        dma((1,)),
        dma((last + 1,)),
        *[dma((3,))] * 4,
        *[dma((2,))] * 5,
    ]
    kept, came, log_weight = pl.pallas_call(
        functools.partial(kernel, nz, ny),
        out_shape=(
            jax.ShapeDtypeStruct((count, half_cols), BF16),
            jax.ShapeDtypeStruct((count, half_cols), BF16),
            jax.ShapeDtypeStruct((heads, count), F32),
        ),
        in_specs=[hbm] * (len(whole) + len(shards) + len(gains)),
        out_specs=(vmem, vmem, vmem),
        scratch_shapes=scratch,
        compiler_params=pltpu.CompilerParams(
            collective_id=0, has_side_effects=True, vmem_limit_bytes=60 * 1024 * 1024
        ),
    )(*whole, *shards, *gains)
    return (kept.astype(F32) + came.astype(F32)).astype(BF16), log_weight


def solution(mesh):
    sp = mesh.shape["sp"]
    ny = math.isqrt(sp)
    nz = sp // ny
    in_specs = (
        P(("fs", "sp"), None),
        P(),
        P("sp", None),
        P(),
        P(),
        P(),
        P(),
        P(None, "tp"),
        P(None, "tp"),
        P(None, "tp"),
        P("sp", "tp"),
        P("sp", "tp"),
        P(None, "tp"),
        P("tp"),
        P("tp", "sp"),
        P("tp", "sp"),
    )
    out_specs = (P(("fs", "sp"), "tp"), P("tp", ("fs", "sp")))
    return jax.shard_map(
        functools.partial(per_device, nz, ny), mesh=mesh, in_specs=in_specs, out_specs=out_specs, check_vma=False
    )
```

```python
import functools
import math

import jax
import jax.numpy as jnp
import numpy as np
from jax import lax
from jax.experimental import pallas as pl
from jax.experimental.pallas import tpu as pltpu
from jax.sharding import PartitionSpec as P

NOPE = 128
ROPE = 64
VDIM = 128
KVR = 256
GROUP = 128
GRID_W = 64
EPS = 1e-06
BASE = 10000.0
HALO = 16
NX = 4
F32 = jnp.float32
BF16 = jnp.bfloat16
MESH = pl.DeviceIdType.MESH


def dot(a, b):
    return jnp.dot(a, b, preferred_element_type=F32)


def dot_t(a, b):
    return lax.dot_general(a, b, (((1,), (1,)), ((), ())), preferred_element_type=F32)


def rms(values, gain):
    inv = lax.rsqrt(jnp.mean(values * values, axis=-1, keepdims=True) + EPS)
    return values * inv * gain


def swap(v):
    half = v.shape[-1] // 2
    return jnp.concatenate([v[:, half:], v[:, :half]], axis=-1)


def await_bytes(ref, sem):
    pltpu.make_async_remote_copy(
        src_ref=ref,
        dst_ref=ref,
        send_sem=sem,
        recv_sem=sem,
        device_id={"tp": 1 - lax.axis_index("tp")},
        device_id_type=MESH,
    ).wait_recv()


class Gather:
    def __init__(self, view, nz, ny, z, y, sems, steps):
        self.view, self.size, self.pos = view, (nz, ny), (z, y)
        self.sems, self.steps = sems, steps

    def device(self, axis, k):
        z, y = (k, self.pos[1]) if axis == 0 else (self.pos[0], k)
        return {"sp": z * self.size[1] + y}

    def send(self, ref, k, arrival, where):
        pltpu.make_async_remote_copy(
            src_ref=ref,
            dst_ref=ref,
            send_sem=self.sems.at[k],
            recv_sem=arrival,
            device_id=where,
            device_id_type=MESH,
        ).start()

    def start_first(self):
        z, y = self.pos
        for half in (0, 1):
            axis = 1 - half
            n = self.size[axis]
            for d in range(1, n):
                where = self.device(axis, lax.rem(self.pos[axis] + d, n))
                self.send(self.view.at[z, y, half], 0, self.sems.at[1], where)

    def wait_first(self):
        await_bytes(self.view.at[0, pl.ds(0, self.size[1] - 1)], self.sems.at[1])

    def block(self, half, k, part=None):
        n = self.size[1 - half]
        rows = slice(None) if part is None else pl.ds(part * (n // 2), n // 2)
        return self.view.at[k, rows, 0] if half == 0 else self.view.at[rows, k, 1]

    def ring_block(self, half, way, s, outgoing=False):
        n = self.size[half]
        back = s - 1 if outgoing else s
        k = lax.rem(self.pos[half] - (1 - 2 * way) * back + n, n)
        return self.block(half, k, way if s == n // 2 else None)

    def blocks(self, s):
        if s == 0:
            return [self.block(0, self.pos[0]), self.block(1, self.pos[1])]
        return [self.ring_block(half, way, s) for half in (0, 1) for way in (0, 1)]

    def like(self, s):
        return self.view.at[0] if s in (0, self.size[0] // 2) else self.view.at[pl.ds(0, 2)]

    def start_ring(self, s):
        for half in (0, 1):
            n = self.size[half]
            for way in (0, 1):
                where = self.device(half, lax.rem(self.pos[half] + (1 - 2 * way) + n, n))
                self.send(self.ring_block(half, way, s, True), 2, self.steps.at[s], where)

    def pass_on(self, s, each=None):
        await_bytes(self.like(s), self.steps.at[s])
        if s < self.size[0] // 2:
            self.start_ring(s + 1)
        if each is not None:
            each(s)

    def finish(self):
        n = self.size[0]
        await_bytes(self.view.at[0, pl.ds(0, n - 1)], self.sems.at[0])
        await_bytes(self.view.at[pl.ds(0, n - 1)], self.sems.at[2])


def kernel(
    nz,
    ny,
    tokens_hbm,
    latent_down_hbm,
    rope_down_hbm,
    query_up_hbm,
    key_up_hbm,
    value_up_hbm,
    conv_taps_hbm,
    query_down,
    glu_value,
    glu_gate,
    head_proj,
    channel_proj,
    norm_gain_hbm,
    query_gain_hbm,
    latent_gain_hbm,
    group_gain_hbm,
    inv_freq_hbm,
    kept,
    part_recv,
    log_weight,
    normed4,
    query_w,
    glu_w,
    ch_all,
    keys_all,
    out_all,
    ql_send,
    ql_recv,
    gated,
    wide,
    conv_send,
    conv_recv,
    queries,
    row_max,
    row_sum,
    acc,
    head_out,
    part_send,
    tokens,
    latent_down,
    rope_down,
    query_up,
    key_up,
    value_up,
    conv_taps,
    norm_gain,
    query_gain,
    latent_gain,
    group_gain,
    inv_freq,
    load_sem,
    shard_sem,
    query_sem,
    glu_sems,
    glu_steps,
    ch_sems,
    ch_steps,
    keys_sems,
    keys_steps,
    out_sems,
    out_steps,
    side_send,
    side_recv,
    relay_send,
    relay_recv,
    pair_send,
    pair_recv,
    x_send,
    x_recv,
    xp_send,
    xp_recv,
    ql_sem,
    cv_sem,
    halo_ssem,
    halo_rsem,
    fin_sem,
):
    sp = lax.axis_index("sp")
    x = lax.axis_index("fs")
    c = lax.axis_index("tp")
    z, y = sp // ny, lax.rem(sp, ny)
    other = 1 - c
    count, depth = tokens.shape
    half_rows = count // 2
    heads = key_up.shape[1] // NOPE
    partner = {"tp": other}
    turn = 1 - 2 * c
    behind, ahead, far = lax.rem(x - turn + NX, NX), lax.rem(x + turn + NX, NX), lax.rem(x + 2, NX)

    barrier = pltpu.get_barrier_semaphore()

    def greet(**where):
        pl.semaphore_signal(barrier, inc=1, device_id=where, device_id_type=MESH)

    for d in range(1, ny):
        greet(sp=z * ny + lax.rem(y + d, ny))
    for d in range(1, nz):
        greet(sp=lax.rem(z + d, nz) * ny + y)
    for d in range(1, NX):
        greet(fs=lax.rem(x + d, NX))
    greet(tp=other)
    has_low = sp > 0
    has_high = sp < nz * ny - 1

    @pl.when(has_low)
    def _():
        greet(sp=sp - 1)

    @pl.when(has_high)
    def _():
        greet(sp=sp + 1)

    first_core = c == 0
    a_pos, b_pos = jnp.where(first_core, z, y), jnp.where(first_core, y, z)
    columns = pl.ds(pl.multiple_of(x * GROUP, GROUP), GROUP)
    slots = (
        (query_down.at[c, :, columns], query_w.at[c, a_pos, b_pos]),
        (glu_value.at[:, :, columns], glu_w.at[z, y, :, :, pl.ds(0, GROUP)]),
        (glu_gate.at[:, :, columns], glu_w.at[z, y, :, :, pl.ds(GROUP, GROUP)]),
        (channel_proj.at[:, :, columns], ch_all.at[x, z, y]),
        (head_proj, out_all.at[z, y]),
    )
    wanted = (
        (tokens_hbm, tokens),
        (latent_down_hbm, latent_down),
        (rope_down_hbm, rope_down),
        (query_up_hbm, query_up),
        (key_up_hbm, key_up),
        (value_up_hbm, value_up),
        (conv_taps_hbm, conv_taps),
        (norm_gain_hbm, norm_gain),
        (query_gain_hbm, query_gain),
        (latent_gain_hbm, latent_gain),
        (group_gain_hbm, group_gain),
        (inv_freq_hbm, inv_freq),
    )
    loads = [pltpu.make_async_copy(a, b, load_sem.at[k]) for k, (a, b) in enumerate(wanted)]
    shards = [pltpu.make_async_copy(a, b, shard_sem.at[k]) for k, (a, b) in enumerate(slots)]
    for copy in shards + loads:
        copy.start()

    g_glu = Gather(glu_w, nz, ny, z, y, glu_sems, glu_steps)
    g_ch = Gather(ch_all.at[x], nz, ny, z, y, ch_sems, ch_steps)
    g_keys = Gather(keys_all.at[c], nz, ny, z, y, keys_sems, keys_steps)
    g_out = Gather(out_all, nz, ny, z, y, out_sems, out_steps)
    sent = []

    def send(src, dst, ssem, rsem, where):
        copy = pltpu.make_async_remote_copy(
            src_ref=src, dst_ref=dst, send_sem=ssem, recv_sem=rsem, device_id=where, device_id_type=MESH
        )
        copy.start()
        return copy

    def arrived(dst, ssem, rsem):
        pltpu.make_async_remote_copy(
            src_ref=dst, dst_ref=dst, send_sem=ssem, recv_sem=rsem, device_id=partner, device_id_type=MESH
        ).wait_recv()

    for copy in shards:
        copy.wait()
    edges = has_low.astype(jnp.int32) + has_high.astype(jnp.int32)
    pl.semaphore_wait(barrier, (ny - 1) + (nz - 1) + (NX - 1) + 1 + edges)

    def query_start(phase):
        for d in range(1, ny):
            if phase == 0:
                a, b = a_pos, lax.rem(b_pos + d, ny)
                ref = query_w.at[c, a_pos, b_pos]
            else:
                a, b = lax.rem(a_pos + d, nz), b_pos
                ref = query_w.at[c, a_pos]
            where = {"sp": jnp.where(first_core, a * ny + b, b * ny + a)}
            send(ref, ref, query_sem.at[2 * phase], query_sem.at[2 * phase + 1], where)

    query_start(0)
    g_glu.start_first()
    g_ch.start_first()
    loads[0].wait()
    loads[7].wait()
    gain = norm_gain[...].astype(F32)[None, :]
    chunk = 32
    for k in range(count // chunk):
        rows = tokens[k * chunk : (k + 1) * chunk, :].astype(F32)
        value = rms(rows, gain).astype(BF16)
        which, first = divmod(k * chunk, half_rows)
        normed4[x, which, first : first + chunk, :] = value

    for way in (0, 1):
        mine = normed4.at[x, c]
        where = {"fs": lax.rem(x + (1 - 2 * way) + NX, NX)}
        sent.append(send(mine, mine, x_send.at[way], x_recv.at[way], where))
    at_row = lax.broadcasted_iota(jnp.int32, (count, ROPE), 0)
    lane = lax.broadcasted_iota(jnp.int32, (count, ROPE), 1)
    place = at_row + sp * count
    grid_row = (place // GRID_W).astype(F32)
    grid_col = lax.rem(place, GRID_W).astype(F32)
    loads[11].wait()
    angles = jnp.where(lax.rem(lane, ROPE // 2) < ROPE // 4, grid_row, grid_col) * inv_freq[...]
    wide[0, 0:count, 0:ROPE] = jnp.cos(angles)
    wide[1, 0:count, 0:ROPE] = jnp.sin(angles) * jnp.where(lane < ROPE // 2, -1.0, 1.0)

    loads[1].wait()
    loads[2].wait()
    loads[9].wait()
    own = normed4[x, c]
    latent = rms(dot(own, latent_down[...]), latent_gain[...].astype(F32)[None, :]).astype(BF16)
    rope_key = dot_t(own, rope_down[...])
    first = pl.multiple_of(c * half_rows, half_rows)
    rope_key = rope_key * wide[0, pl.ds(first, half_rows), 0:ROPE] + swap(rope_key) * wide[
        1, pl.ds(first, half_rows), 0:ROPE
    ]
    quarter = half_rows // 2
    rope_pair = jnp.concatenate([rope_key[:quarter], rope_key[quarter:]], axis=1).astype(BF16)
    for h in (0, 1):
        lo = h * (quarter // 2)
        hi = lo + quarter // 2
        keys_all[c, z, y, h, :, 0:KVR] = latent[lo:hi]
        keys_all[c, z, y, h, :, KVR : 2 * KVR] = latent[quarter + lo : quarter + hi]
        keys_all[c, z, y, h, :, 2 * KVR :] = rope_pair[lo:hi]

    g_keys.start_first()
    for copy in loads[3:7] + [loads[8], loads[10]]:
        copy.wait()

    def pair_keys(s):
        for block in g_keys.blocks(s):
            send(block, block, pair_send.at[0], pair_recv.at[s], partner)

    def pair_arrived(s):
        await_bytes(g_keys.like(s), pair_recv.at[s])

    def share(s):
        for block in g_ch.blocks(s):
            for w in (0, 1):
                where = {"fs": lax.rem(x + (1 - 2 * w) + NX, NX)}
                send(block, block, side_send.at[0], side_recv.at[w, s], where)

    passing = Gather(ch_all.at[behind], nz, ny, z, y, ch_sems, ch_steps)

    def relay(s):
        await_bytes(g_ch.like(s), side_recv.at[c, s])
        for block in passing.blocks(s):
            send(block, block, relay_send.at[0], relay_recv.at[s], {"fs": ahead})

    await_bytes(query_w.at[0, 0, pl.ds(0, ny - 1)], query_sem.at[1])
    query_start(1)
    g_out.start_first()

    last = nz // 2
    g_glu.wait_first()
    g_glu.start_ring(1)
    g_ch.wait_first()
    g_ch.start_ring(1)

    for way in (0, 1):
        src = lax.rem(x - (1 - 2 * way) + NX, NX)
        piece = normed4.at[src, c]
        arrived(piece, x_send.at[way], x_recv.at[way])
        sent.append(send(piece, piece, xp_send.at[way], xp_recv.at[way], partner))
    onward = normed4.at[behind, c]
    sent.append(send(onward, onward, x_send.at[2], x_recv.at[2], {"fs": ahead}))

    g_keys.wait_first()
    g_keys.start_ring(1)
    pair_keys(0)

    g_out.wait_first()
    g_out.start_ring(1)

    await_bytes(query_w.at[0, pl.ds(0, nz - 1)], query_sem.at[3])
    sent.append(send(query_w.at[c], query_w.at[c], query_sem.at[4], query_sem.at[5], partner))
    piece = normed4.at[far, c]
    arrived(piece, x_send.at[2], x_recv.at[2])
    sent.append(send(piece, piece, xp_send.at[2], xp_recv.at[2], partner))
    g_glu.pass_on(1)
    g_ch.pass_on(1)

    def to_parts(src, dst, sems):
        for d in range(1, NX):
            part = lax.rem(x + d, NX)
            send(src.at[part], dst.at[x], sems.at[0], sems.at[1], {"fs": part})

    def from_parts(dst, sems):
        await_bytes(dst.at[pl.ds(0, NX - 1)], sems.at[1])

    await_bytes(query_w.at[other], query_sem.at[5])
    for k in range(3):
        src = far if k == 2 else lax.rem(x - (1 - 2 * k) + NX, NX)
        arrived(normed4.at[src, other], xp_send.at[k], xp_recv.at[k])
    pieces = []
    for row in range(nz):
        for column in range(ny):
            pieces += [query_w[0, row, column], query_w[1, column, row]]
    everyone = normed4[...].reshape(NX * count, depth)
    ql_send[...] = dot(everyone, jnp.concatenate(pieces, axis=0)).reshape(NX, count, GROUP)
    to_parts(ql_send, ql_recv, ql_sem)
    ql_recv[x] = ql_send[x]
    share(0)
    share(1)

    g_keys.pass_on(1, pair_keys)

    from_parts(ql_recv, ql_sem)
    latent_query = jnp.concatenate([ql_recv[k] for k in range(NX)], axis=1)
    latent_query = rms(latent_query, query_gain[...].astype(F32)[None, :]).astype(BF16)
    query_all = dot(latent_query, query_up[...])
    cosine = wide[0, 0:count, 0:ROPE]
    sine = wide[1, 0:count, 0:ROPE]
    nothing = jnp.zeros((count, ROPE), F32)
    for h in range(heads):
        start = h * (NOPE + ROPE)
        plain = query_all[:, start : start + NOPE].astype(BF16)
        turned = query_all[:, start + NOPE : start + NOPE + ROPE]
        turned = turned * cosine + swap(turned) * sine
        absorbed = dot_t(plain, key_up[:, h * NOPE : (h + 1) * NOPE]).astype(BF16)
        rows = slice(h * count, (h + 1) * count)
        queries[0, rows, 0:KVR] = absorbed
        queries[1, rows, 0:KVR] = absorbed
        queries[0, rows, KVR:] = jnp.concatenate([turned, nothing], axis=1).astype(BF16)
        queries[1, rows, KVR:] = jnp.concatenate([nothing, turned], axis=1).astype(BF16)

    scale = (NOPE + ROPE) ** (-0.5)
    factor = scale * math.log2(math.e)
    row_max[...] = jnp.full(row_max.shape, -1e30, F32)
    row_sum[...] = jnp.zeros(row_sum.shape, F32)
    acc[...] = jnp.zeros(acc.shape, F32)
    lines = quarter // 2

    def attend(k, carry):
        odd = lax.rem(k, 2)
        step = odd * (lax.div(k, 2) + 1) - (1 - odd) * lax.div(k, 2)
        row = lax.rem(z + step + nz, nz)
        column = lax.rem(y + step + ny, ny)
        pieces, values = [], []
        for core in (0, 1):
            upper = keys_all[core, row, :, 0].reshape(ny * lines, 2 * KVR + 2 * ROPE)
            lower = keys_all[core, :, column, 1].reshape(nz * lines, 2 * KVR + 2 * ROPE)
            block = jnp.concatenate([upper, lower], axis=0)
            tail = block[:, 2 * KVR :]
            for low in (0, 1):
                value = block[:, low * KVR : (low + 1) * KVR]
                pieces.append((low, jnp.concatenate([value, tail], axis=1)))
                values.append(value)
        size = row_max.shape[0] // 2
        parts = [slice(p * size, (p + 1) * size) for p in range(2)]
        wide_scores = [jnp.concatenate([dot_t(queries[low, rows], piece) for low, piece in pieces], axis=1) for rows in parts]
        stacked = jnp.concatenate(values, axis=0)
        for rows, scores in zip(parts, wide_scores):
            before = row_max[rows]
            now = jnp.maximum(before, jnp.max(scores, axis=1, keepdims=True))
            shrink = jnp.exp2((before - now) * factor)
            weights = jnp.exp2((scores - jnp.tile(now, (1, scores.shape[1] // 128))) * factor)
            row_sum[rows] = row_sum[rows] * shrink + jnp.sum(weights, axis=1, keepdims=True)
            row_max[rows] = now
            acc[rows] = acc[rows] * jnp.tile(shrink, (1, KVR // 128)) + dot(weights.astype(BF16), stacked)
        return carry

    g_glu.pass_on(2)
    g_ch.pass_on(2, share)
    g_out.pass_on(1)
    pair_arrived(0)
    lax.fori_loop(0, 1, attend, 0)
    pair_arrived(1)
    g_keys.pass_on(2, pair_keys)
    lax.fori_loop(1, 2, attend, 0)
    g_glu.pass_on(3)
    g_ch.pass_on(3, share)
    relay(0)
    relay(1)
    lax.fori_loop(2, 3, attend, 0)
    g_out.pass_on(2)
    pair_arrived(2)
    lax.fori_loop(3, 5, attend, 0)

    g_keys.pass_on(3, pair_keys)
    g_glu.pass_on(4)
    g_ch.pass_on(4, share)
    relay(2)
    glu_weights = glu_w[...].reshape(depth, 2 * GROUP)
    for j in range(NX):
        product = dot(normed4[j].reshape(count, depth), glu_weights)
        gated[j, HALO : HALO + count, :] = (product[:, :GROUP] * jax.nn.sigmoid(product[:, GROUP:])).astype(BF16)

    low_src, high_src = gated.at[:, pl.ds(HALO, HALO)], gated.at[:, pl.ds(count, HALO)]
    low_dst, high_dst = gated.at[:, pl.ds(0, HALO)], gated.at[:, pl.ds(HALO + count, HALO)]

    def halo_copy(up):
        src, dst = (high_src, low_dst) if up else (low_src, high_dst)
        k = 0 if up else 1
        return pltpu.make_async_remote_copy(
            src_ref=src,
            dst_ref=dst,
            send_sem=halo_ssem.at[k],
            recv_sem=halo_rsem.at[k],
            device_id={"sp": sp + 1 if up else sp - 1},
            device_id_type=MESH,
        )

    @pl.when(has_high)
    def _():
        halo_copy(True).start()

    @pl.when(has_low)
    def _():
        halo_copy(False).start()

    edge = jnp.zeros((NX, HALO, GROUP), BF16)

    @pl.when(jnp.logical_not(has_low))
    def _():
        gated[:, 0:HALO, :] = edge

    @pl.when(jnp.logical_not(has_high))
    def _():
        gated[:, HALO + count :, :] = edge

    relay(3)
    pair_arrived(3)
    lax.fori_loop(5, 6, attend, 0)
    g_out.pass_on(3)

    @pl.when(has_low)
    def _():
        halo_copy(True).wait_recv()

    @pl.when(has_high)
    def _():
        halo_copy(False).wait_recv()

    reach = conv_taps.shape[0] // 2
    taps = conv_taps[:, columns].astype(F32)
    gains = group_gain[...].astype(F32)[None, :]
    channel_gain = gains[:, :GROUP]
    for k in range(1, NX):
        channel_gain = jnp.where(x == k, gains[:, k * GROUP : (k + 1) * GROUP], channel_gain)
    for j in range(NX):
        wide[j, :, :] = gated[j].astype(F32)
        total = jnp.zeros((count, GROUP), F32)
        for t in range(2 * reach + 1):
            lo = HALO - reach + t
            total = total + wide[j, lo : lo + count, :] * taps[t : t + 1, :]
        centred = total - jnp.mean(total, axis=-1, keepdims=True)
        spread = jnp.mean(centred * centred, axis=-1, keepdims=True)
        conv_send[j] = jax.nn.silu(centred * lax.rsqrt(spread + EPS) * channel_gain).astype(BF16)
    to_parts(conv_send, conv_recv, cv_sem)
    conv_recv[x] = conv_send[x]

    g_keys.pass_on(4, pair_keys)
    relay(4)
    lax.fori_loop(6, 7, attend, 0)
    pair_arrived(4)
    lax.fori_loop(7, 8, attend, 0)

    for h in range(heads):
        rows = slice(h * count, (h + 1) * count)
        attended = (acc[rows, :] / jnp.tile(row_sum[rows, :], (1, KVR // 128))).astype(BF16)
        head_out[:, h * VDIM : (h + 1) * VDIM] = dot(attended, value_up[:, h * VDIM : (h + 1) * VDIM]).astype(BF16)
        logs = row_max[rows, :] * scale + jnp.log(row_sum[rows, :])
        log_weight[h : h + 1, :] = jnp.transpose(logs)[0:1, :]

    from_parts(conv_recv, cv_sem)
    mixed = jnp.concatenate([head_out[...]] + [conv_recv[k] for k in range(NX)], axis=1)
    zs = nz // 2
    width = zs * ny * 2 * out_all.shape[3]
    g_out.pass_on(4)
    for s in range(last + 1):
        await_bytes(g_ch.like(s), side_recv.at[other, s])
        await_bytes(g_ch.like(s), relay_recv.at[s])

    def columns_of(core):
        rows = pl.ds(core * zs, zs)
        parts = [out_all[rows].reshape(width, heads * VDIM)]
        parts += [ch_all[k, rows].reshape(width, GROUP) for k in range(NX)]
        return dot_t(mixed, jnp.concatenate(parts, axis=1)).astype(BF16)

    part_send[...] = columns_of(other)
    sent.append(send(part_send, part_recv, fin_sem.at[0], fin_sem.at[1], partner))
    kept[...] = columns_of(c)
    arrived(part_recv, fin_sem.at[0], fin_sem.at[1])

    for copy in sent:
        copy.wait_send()
    await_bytes(query_w.at[0, 0, pl.ds(0, ny - 1)], query_sem.at[0])
    await_bytes(query_w.at[0, pl.ds(0, nz - 1)], query_sem.at[2])
    await_bytes(keys_all.at[0], pair_send.at[0])
    await_bytes(ch_all.at[pl.ds(0, 2)], side_send.at[0])
    await_bytes(ch_all.at[0], relay_send.at[0])
    await_bytes(ql_send.at[pl.ds(0, NX - 1)], ql_sem.at[0])
    await_bytes(conv_send.at[pl.ds(0, NX - 1)], cv_sem.at[0])
    g_glu.finish()
    g_ch.finish()
    g_keys.finish()
    g_out.finish()

    @pl.when(has_high)
    def _():
        halo_copy(True).wait_send()

    @pl.when(has_low)
    def _():
        halo_copy(False).wait_send()


def add_up(kept, came, logs, out, log_weight):
    out[...] = (kept[...].astype(F32) + came[...].astype(F32)).astype(BF16)
    log_weight[...] = logs[...]


def per_device(
    nz,
    ny,
    tokens,
    norm_gain,
    query_down,
    query_gain,
    latent_down,
    latent_gain,
    rope_down,
    query_up,
    key_up,
    value_up,
    glu_value,
    glu_gate,
    conv_taps,
    group_gain,
    head_proj,
    channel_proj,
):
    count, depth = tokens.shape
    heads = key_up.shape[1] // NOPE

    def halves(a):
        return a.reshape(2, a.shape[0] // 2, a.shape[1])

    freq = (BASE ** (-np.arange(ROPE // 4, dtype=np.float64) / (ROPE // 4))).astype(np.float32)
    whole = (tokens, latent_down, rope_down.T, query_up, key_up, value_up, conv_taps)
    shards = [halves(a) for a in (query_down, glu_value, glu_gate, head_proj.T, channel_proj.T)]
    gains = (norm_gain, query_gain, latent_gain, group_gain, jnp.asarray(np.tile(freq, 4)[None, :]))
    shard = query_down.shape[0] // 2
    out_cols = head_proj.shape[1]
    half_cols = nz * ny * out_cols // 2
    last = nz // 2
    dma = pltpu.SemaphoreType.DMA
    vmem = pl.BlockSpec(memory_space=pltpu.VMEM)
    hbm = pl.BlockSpec(memory_space=pltpu.HBM)

    def buf(*shape, dtype=BF16):
        return pltpu.VMEM(shape, dtype)

    scratch = [
        buf(NX, 2, count // 2, depth),
        buf(2, nz, ny, shard, GROUP),
        buf(nz, ny, 2, shard, 2 * GROUP),
        buf(NX, nz, ny, 2, out_cols // 2, GROUP),
        buf(2, nz, ny, 2, count // 8, 2 * KVR + 2 * ROPE),
        buf(nz, ny, 2, out_cols // 2, heads * VDIM),
        buf(NX, count, GROUP, dtype=F32),
        buf(NX, count, GROUP, dtype=F32),
        buf(NX, count + 2 * HALO, GROUP),
        buf(NX, count + 2 * HALO, GROUP, dtype=F32),
        buf(NX, count, GROUP),
        buf(NX, count, GROUP),
        buf(2, heads * count, KVR + 2 * ROPE),
        buf(heads * count, 128, dtype=F32),
        buf(heads * count, 128, dtype=F32),
        buf(heads * count, KVR, dtype=F32),
        buf(count, heads * VDIM),
        buf(count, half_cols),
        *[buf(*a.shape, dtype=a.dtype) for a in whole + gains],
        dma((len(whole + gains),)),
        dma((5,)),
        dma((6,)),
        *[dma((3,)), dma((last + 1,))] * 4,
        dma((1,)),
        dma((2, last + 1)),
        dma((1,)),
        dma((last + 1,)),
        dma((1,)),
        dma((last + 1,)),
        *[dma((3,))] * 4,
        *[dma((2,))] * 5,
    ]
    kept, came, log_weight = pl.pallas_call(
        functools.partial(kernel, nz, ny),
        out_shape=(
            jax.ShapeDtypeStruct((count, half_cols), BF16),
            jax.ShapeDtypeStruct((count, half_cols), BF16),
            jax.ShapeDtypeStruct((heads, count), F32),
        ),
        in_specs=[hbm] * (len(whole) + len(shards) + len(gains)),
        out_specs=(vmem, vmem, vmem),
        scratch_shapes=scratch,
        compiler_params=pltpu.CompilerParams(
            collective_id=0, has_side_effects=True, vmem_limit_bytes=60 * 1024 * 1024
        ),
    )(*whole, *shards, *gains)
    return pl.pallas_call(
        add_up,
        out_shape=(jax.ShapeDtypeStruct(kept.shape, BF16), jax.ShapeDtypeStruct(log_weight.shape, F32)),
        in_specs=[vmem] * 3,
        out_specs=(vmem, vmem),
    )(kept, came, log_weight)


def solution(mesh):
    sp = mesh.shape["sp"]
    ny = math.isqrt(sp)
    nz = sp // ny
    in_specs = (
        P(("fs", "sp"), None),
        P(),
        P("sp", None),
        P(),
        P(),
        P(),
        P(),
        P(None, "tp"),
        P(None, "tp"),
        P(None, "tp"),
        P("sp", "tp"),
        P("sp", "tp"),
        P(None, "tp"),
        P("tp"),
        P("tp", "sp"),
        P("tp", "sp"),
    )
    out_specs = (P(("fs", "sp"), "tp"), P("tp", ("fs", "sp")))
    return jax.shard_map(
        functools.partial(per_device, nz, ny), mesh=mesh, in_specs=in_specs, out_specs=out_specs, check_vma=False
    )
```
